32 devices in a mesh: grp: 2 (over x), ep: 16 (over z, y, core).
Axes of the slice: x: 2, y: 2, z: 4, core: 2. Of those that a mesh axis runs over, the one named last changes fastest.
Arguments:
- tokens: bfloat16 [256, 2048], P(('grp', 'ep')), parts along dimension 0, may hold values from -24 to 24
- norm_gain: bfloat16 [2048], replicated, may hold values from 0.099609375 to 1.8984375
- w_query: bfloat16 [2048, 512], P('ep'), may hold values from -0.1875 to 0.1875
- w_key: bfloat16 [2048, 128], replicated, may hold values from -0.125 to 0.125
- w_value: bfloat16 [2048, 128], replicated, may hold values from -0.125 to 0.125
- w_out: bfloat16 [512, 2048], P(None, 'ep'), may hold values from -1 to 1
- cache_k: bfloat16 [256, 1024, 128], P(('grp', 'ep')), parts along dimension 0, may hold values from -6 to 6
- cache_v: bfloat16 [256, 1024, 128], P(('grp', 'ep')), parts along dimension 0, may hold values from -6 to 6
- head_offset: float32 [8], replicated, may hold values from -12 to -3
- key_shift: float32 [256, 2, 1024], P(('grp', 'ep')), parts along dimension 0, may hold values from -3 to 9
- lengths: int32 [256], P(('grp', 'ep')), parts along dimension 0, may hold values from 1 to 1024, 65536 in all
- moe_gain: bfloat16 [2048], replicated, may hold values from 0.099609375 to 1.8984375
- route_ids: int32 [256, 6], P(('grp', 'ep')), parts along dimension 0, may hold values from 0 to 15, all different within a row; in each aligned block of 8 rows (0 to 7, 8 to 15, ...) at most 6 rows name the same one
- route_score: float32 [256, 6], P(('grp', 'ep')), parts along dimension 0, may hold values from 0.05 to 1
- w_gate: bfloat16 [16, 2048, 256], P('ep'), may hold values from -0.125 to 0.125
- w_up: bfloat16 [16, 2048, 256], P('ep'), may hold values from -0.125 to 0.125
- w_down: bfloat16 [16, 256, 2048], P('ep'), may hold values from -0.375 to 0.375
- shared_gate: bfloat16 [2048, 256], replicated, may hold values from -0.125 to 0.125
- shared_up: bfloat16 [2048, 256], replicated, may hold values from -0.125 to 0.125
- shared_down: bfloat16 [256, 2048], replicated, may hold values from -0.375 to 0.375
Outputs:
- out: bfloat16 [256, 2048], P(('grp', 'ep')), parts along dimension 0
- new_key: bfloat16 [256, 128], P(('grp', 'ep')), parts along dimension 0
- new_value: bfloat16 [256, 128], P(('grp', 'ep')), parts along dimension 0
The draws below stay inside these ranges and needn't reach their ends.
There are 2 independent parts, one for each index of `grp`. The reference program is written for one: setup_inputs(seed, part) draws one part's arguments, and reference() takes and returns one part's arrays. A program takes and returns all parts, laid end to end along the dimension named above; an argument that names none is the same for every part. Nothing has to cross between parts.
Inputs may be any that keep to these rules, and one draw needn't show every extreme that they name: Each sequence's cache holds lengths[b] past positions at the start; the new token stands at position lengths[b]. Some sequence of every part has exactly 1024. `route_ids`: the 6 experts of a token differ. Among the tokens of one device, no expert is named more than 6 times, a bound that some block reaches in every draw.
All inputs are finite; a program needn't handle non-finite values. No bound on the sum of `lengths` on one device may be relied on, other than what follows from the above.
Results may differ from the reference program's by a relative error of at most 0.0069.
Values may be sent and summed in bfloat16 or wider, within the bound.
A program may use at most 64 MiB of HBM per device.

```python
import math
import jax
import jax.numpy as jnp
import numpy as np
from jax import lax

D = 2048
QH = 8
KVH = 2
F = 256
SF = 256
TOPK = 6
SEQ_DEV = 8
STORED_PLACES = 1024
QW = 512
KVW = 128
EXPERTS = 16
STRING_COUNT = 128
CAP = 6
N_EP = 16


def draw_tokens(key, part):
    key_one = jax.random.fold_in(key, 0)
    extra_lookup_vector = jax.random.fold_in(key, 2)
    raw_draw = jax.random.truncated_normal(key_one, -4.0, 4.0, (STRING_COUNT, D), jnp.float32)
    scales = jnp.exp(jax.random.uniform(extra_lookup_vector, (STRING_COUNT, 1), jnp.float32, math.log(0.3), math.log(3.0)))
    drawn = raw_draw * scales
    return drawn.astype(jnp.bfloat16)


def draw_head_offset(key, part):
    key_one, key_two, extra_lookup_vector = jax.random.split(key, 3)
    head_rank = jax.random.permutation(key_one, QH)
    fast_rate = jax.random.uniform(key_two, (QH,), jnp.float32, -4.5, -3.5)
    slow_rate = -math.log(STORED_PLACES) - jax.random.uniform(extra_lookup_vector, (QH,), jnp.float32, 0.3, 0.9)
    is_fast = head_rank < QH // 2
    return jnp.where(is_fast, fast_rate, slow_rate)


def draw_key_shift(key, part):
    key_one, key_two, extra_lookup_vector = jax.random.split(key, 3)
    string_level = jax.random.uniform(key_one, (STRING_COUNT, 1, 1), jnp.float32, -0.7, 0.7)
    rough_fraction = 0.4 * jax.random.truncated_normal(key_two, -3.0, 3.0, (STRING_COUNT, KVH, STORED_PLACES), jnp.float32)
    spike_index = jax.random.randint(extra_lookup_vector, (STRING_COUNT, 1, 1, 3), 0, STORED_PLACES)
    place_destinations = jnp.arange(STORED_PLACES, dtype=jnp.int32)
    spike_marker = jnp.any(place_destinations[None, None, :, None] == spike_index, axis=3).astype(jnp.float32)
    return string_level + rough_fraction + 6.5 * spike_marker


def with_spikes(array, own_key, source, target, blocks, factor):
    def block_of(position):
        return (jnp.arange(array.shape[position]) // (array.shape[position] // blocks)).reshape((-1,) + (1,) * (array.ndim - 1 - position))

    first = jax.random.permutation(own_key, blocks)[block_of(target)]
    second = (block_of(target) + blocks // 2) % blocks
    return jnp.where((block_of(source) == first) | (block_of(source) == second), factor * array, array)


def level_of(rng, extent, cuts, least, largest):
    def one(position, parts):
        steps = jax.random.uniform(jax.random.fold_in(jax.random.fold_in(rng, 6), position), (parts,), jnp.float32, least / len(cuts), largest / len(cuts))
        return jnp.repeat(jnp.exp(steps), extent[position] // parts).reshape((-1,) + (1,) * (len(extent) - position - 1))

    loudness = one(*cuts[0])
    for cut in cuts[1:]:
        loudness = loudness * one(*cut)
    return loudness


def length_profile(number_of, total, bound, skew):
    portions = [(1 << 20) // math.isqrt(grade ** skew) + 1 for grade in range(2, number_of + 1)]
    spare, holding = total - bound - (number_of - 1), [1] * (number_of - 1)
    while spare > 0:
        free = [i for i in range(number_of - 1) if holding[i] < bound]
        pool, budget = sum([portions[i] for i in free]), spare
        for i in free:
            addition = min(bound - holding[i], max(1, budget * portions[i] // pool), spare)
            holding[i] = holding[i] + addition
            spare = spare - addition
    return np.array([bound] + holding)


def ragged_sizes(key, number_of, total, most, skew):
    if number_of == 2:
        one = jax.random.randint(key, (), max(1, total - most), min(most, total - 1) + 1)
        return jnp.stack([one, total - one])
    tallies = jnp.asarray(length_profile(number_of, total, most, skew), jnp.int32)
    pairs = (number_of - 1) // 2
    donor, sink = tallies[1:1 + 2 * pairs:2], tallies[2:2 + 2 * pairs:2]
    room = jnp.minimum(donor - 1, most - sink)
    passed = jax.random.randint(jax.random.fold_in(key, 1), (pairs,), 0, 1 << 20) % (room + 1)
    tallies = tallies.at[1:1 + 2 * pairs:2].set(donor - passed).at[2:2 + 2 * pairs:2].set(sink + passed)
    return tallies[jax.random.permutation(jax.random.fold_in(key, 2), number_of)]


def routed_block(own_key, own, number, rows, count, top, most, lean):
    sequence = jax.random.permutation(own_key, count)
    packed, usual = portions_of(count, rows * top, most, lean, True), portions_of(count, rows * top, most, lean, False)
    places = jnp.arange(count)

    def named(sizes, turn):
        used = int((sizes > 0).sum())
        fixed = max(1, used // 4)
        shifted = fixed + (places - fixed + turn * (used - fixed)) % max(1, count - fixed)
        return jnp.zeros((count,), jnp.int32).at[sequence[jnp.where(places < fixed, places, shifted)]].set(jnp.asarray(sizes, jnp.int32))

    sizes = jnp.where(number % 4 == 0, named(packed, number // 4), named(usual, number - number // 4 - 1))
    mixed = jax.random.permutation(jax.random.fold_in(own, 3), count)
    giver, receiver = mixed[0:count // 2 * 2:2], mixed[1:count // 2 * 2:2]
    margin = jnp.minimum(sizes[giver] - 1, most - sizes[receiver]) // 2
    margin = jnp.where((giver == sequence[0]) | (receiver == sequence[0]) | (sizes[receiver] == 0), 0, jnp.maximum(margin, 0))
    shifted = jax.random.randint(jax.random.fold_in(own, 4), (count // 2,), 0, 1 << 20) % (margin + 1)
    sizes = sizes.at[giver].add(-shifted).at[receiver].add(shifted)
    items = jnp.searchsorted(jnp.cumsum(sizes), jnp.arange(rows * top), side="right").astype(jnp.int32)
    listing = items.reshape(top, rows).T
    listing = listing[jax.random.permutation(jax.random.fold_in(own, 1), rows)]
    turn = jax.random.randint(jax.random.fold_in(own, 2), (rows, 1), 0, top)
    return jnp.take_along_axis(listing, (jnp.arange(top)[None, :] + turn) % top, axis=1)


def portions_of(number_of, total, limit, skew, full):
    weights = [(1 << 20) // math.isqrt(grade ** skew) + 1 for grade in range(1, number_of + 1)]
    largest = limit if full else min(limit, max(-(-total // number_of), total * weights[0] // sum(weights)))
    least = 1 if total - largest >= number_of - 1 else 0
    given, spare = [largest] + [least] * (number_of - 1), total - largest - least * (number_of - 1)
    while spare > 0:
        free = [i for i in range(1, number_of) if given[i] < largest] or [i for i in range(1, number_of) if given[i] < limit]
        mass, left = sum([weights[i] for i in free]), spare
        for i in free:
            more = min(limit - given[i], max(1, left * weights[i] // mass), spare)
            given[i] = given[i] + more
            spare = spare - more
    return np.array(given)


def noise(key, dims, scale, reach, cuts=(), kind=jnp.bfloat16):
    array = jax.random.normal(key, dims, jnp.float32) * scale
    if len(cuts) > 0:
        array = level_of(key, dims, cuts, -0.22, 0.18) * array
    return jnp.clip(array, min=-reach, max=reach).astype(kind)


def bell_draw_with(rng, shape, width, limit, cuts, heavy, held_as=jnp.bfloat16):
    array = width * jax.random.normal(rng, shape, jnp.float32)
    if cuts:
        array = array * level_of(rng, shape, cuts, -0.22, 0.18)
    return jnp.clip(with_spikes(array, jax.random.fold_in(rng, 3), *heavy), -limit, limit).astype(held_as)


def setup_inputs(seed: int = 0, part: int = 0) -> dict:
    key_of = jax.random.split(jax.random.key(seed), 21)
    part_keys = jax.random.split(jax.random.fold_in(key_of[20], part), 21)
    tokens = draw_tokens(jax.random.fold_in(jax.random.fold_in(key_of[20], part), 71), part)
    norm_gain = jnp.clip(1.0 + 0.18 * jax.random.normal(key_of[1], (D,), jnp.float32), 0.099609375, 1.8984375).astype(jnp.bfloat16)
    w_query = bell_draw_with(key_of[2], (D, QW), D ** -0.5, 0.1875, ((0, 16),), (0, 1, 16, 2.0))
    w_key = noise(key_of[3], (D, KVW), D ** -0.5, 0.125)
    w_value = noise(key_of[4], (D, KVW), D ** -0.5, 0.125)
    w_out = noise(key_of[5], (QW, D), (QW // 16) ** -0.5, 1.0, ((1, 16),))
    cache_k = noise(part_keys[6], (STRING_COUNT, STORED_PLACES, KVW), 1.0, 6.0, ((0, 16),))
    cache_v = noise(part_keys[7], (STRING_COUNT, STORED_PLACES, KVW), 1.0, 6.0, ((0, 16),))
    head_offset = draw_head_offset(jax.random.fold_in(key_of[20], 71), part)
    key_shift = draw_key_shift(jax.random.fold_in(jax.random.fold_in(key_of[20], part), 71), part)
    lengths = ragged_sizes(part_keys[10], STRING_COUNT, STRING_COUNT * STORED_PLACES // 2, STORED_PLACES, 2).astype(jnp.int32)
    moe_gain = jnp.clip(1.0 + 0.18 * jax.random.normal(key_of[11], (D,), jnp.float32), 0.099609375, 1.8984375).astype(jnp.bfloat16)
    route_ids_keys = jax.random.split(jax.random.fold_in(part_keys[12], 1), STRING_COUNT // SEQ_DEV)
    route_ids_turns = jax.random.permutation(jax.random.fold_in(part_keys[12], 3), STRING_COUNT // SEQ_DEV)
    route_ids = jax.vmap(lambda own, number: routed_block(jax.random.fold_in(part_keys[12], 2), own, number, SEQ_DEV, EXPERTS, TOPK, CAP, 2))(route_ids_keys, route_ids_turns).reshape((STRING_COUNT, TOPK))
    route_score = jnp.clip(0.05 + 0.95 * jax.random.uniform(part_keys[13], (STRING_COUNT, TOPK), jnp.float32) ** level_of(part_keys[13], (STRING_COUNT, TOPK), ((0, 16),), -0.2, 0.2), 0.05, 1.0)
    w_gate = noise(key_of[14], (EXPERTS, D, F), D ** -0.5, 0.125, ((0, 16),))
    w_up = noise(key_of[15], (EXPERTS, D, F), D ** -0.5, 0.125, ((0, 16),))
    w_down = noise(key_of[16], (EXPERTS, F, D), F ** -0.5, 0.375, ((0, 16),))
    shared_gate = noise(key_of[17], (D, SF), D ** -0.5, 0.125)
    shared_up = noise(key_of[18], (D, SF), D ** -0.5, 0.125)
    shared_down = noise(key_of[19], (SF, D), SF ** -0.5, 0.375)
    return {"tokens": tokens, "norm_gain": norm_gain, "w_query": w_query, "w_key": w_key, "w_value": w_value, "w_out": w_out, "cache_k": cache_k, "cache_v": cache_v, "head_offset": head_offset, "key_shift": key_shift, "lengths": lengths, "moe_gain": moe_gain, "route_ids": route_ids, "route_score": route_score, "w_gate": w_gate, "w_up": w_up, "w_down": w_down, "shared_gate": shared_gate, "shared_up": shared_up, "shared_down": shared_down}


EPSILON = 1e-06
ROUTED_SCALE = 2.5

def norm_rows(values, gain_vec):
    mean_sq = lax.optimization_barrier(jnp.mean(values * values, axis=-1, keepdims=True))
    return values * lax.rsqrt(mean_sq + EPSILON) * gain_vec.astype(jnp.float32)

def swiglu(row_block, gate_w, up_w, down_w):
    gate_part = jnp.dot(row_block, gate_w, preferred_element_type=jnp.float32)
    up_part = jnp.dot(row_block, up_w, preferred_element_type=jnp.float32)
    hidden = (jax.nn.silu(gate_part) * up_part).astype(jnp.bfloat16)
    return jnp.dot(hidden, down_w, preferred_element_type=jnp.float32)

def stick_weights(logits, offset, shifts, lengths):
    logits = logits + offset[None, :, :, None] + shifts[:, :, None, :]
    place_destinations = jnp.arange(logits.shape[-1], dtype=jnp.int32)
    is_live = place_destinations[None, None, None, :] < lengths.astype(jnp.int32)[:, None, None, None]
    log_fall = jnp.where(is_live, jax.nn.log_sigmoid(-logits), 0.0)
    later_sum = lax.cumsum(log_fall, axis=3, reverse=True) - log_fall
    return jnp.where(is_live, jnp.exp(jax.nn.log_sigmoid(logits) + later_sum), 0.0).astype(jnp.bfloat16)

def attend(queries, cache_k, cache_v, offset, shifts, lengths):
    seq_count, cache_len, kv_width = cache_k.shape
    groups = shifts.shape[1]
    head_dim = kv_width // groups
    per_group = queries.shape[1] // kv_width
    query_heads = queries.astype(jnp.float32).reshape(seq_count, groups, per_group, head_dim)
    key_heads = cache_k.astype(jnp.float32).reshape(seq_count, cache_len, groups, head_dim)
    value_heads = cache_v.astype(jnp.float32).reshape(seq_count, cache_len, groups, head_dim)
    logits = jnp.einsum('sgrd,slgd->sgrl', query_heads, key_heads) / math.sqrt(head_dim)
    weights = stick_weights(logits, offset.reshape(groups, per_group), shifts, lengths)
    mixed_out = jnp.einsum('sgrl,slgd->sgrd', weights.astype(jnp.float32), value_heads)
    return mixed_out.reshape(seq_count, queries.shape[1]).astype(jnp.bfloat16)

def reference(tokens, norm_gain, w_query, w_key, w_value, w_out, cache_k, cache_v, head_offset, key_shift, lengths, moe_gain, route_ids, route_score, w_gate, w_up, w_down, shared_gate, shared_up, shared_down):
    normed = norm_rows(tokens.astype(jnp.float32), norm_gain).astype(jnp.bfloat16)
    queries = jnp.dot(normed, w_query, preferred_element_type=jnp.float32).astype(jnp.bfloat16)
    new_key = jnp.dot(normed, w_key, preferred_element_type=jnp.float32).astype(jnp.bfloat16)
    new_value = jnp.dot(normed, w_value, preferred_element_type=jnp.float32).astype(jnp.bfloat16)
    blocks = STRING_COUNT // SEQ_DEV
    attended = lax.map(lambda pieces: attend(pieces[0], pieces[1], pieces[2], head_offset, pieces[3], pieces[4]), (queries.reshape(blocks, SEQ_DEV, QW), cache_k.reshape(blocks, SEQ_DEV, STORED_PLACES, KVW), cache_v.reshape(blocks, SEQ_DEV, STORED_PLACES, KVW), key_shift.reshape(blocks, SEQ_DEV, KVH, STORED_PLACES), lengths.reshape(blocks, SEQ_DEV))).reshape(STRING_COUNT, QW)
    branch = jnp.dot(attended, w_out, preferred_element_type=jnp.float32).astype(jnp.bfloat16)
    residual = tokens.astype(jnp.float32) + branch.astype(jnp.float32)
    moe_in = norm_rows(residual, moe_gain).astype(jnp.bfloat16)
    route_share = ROUTED_SCALE * route_score / lax.optimization_barrier(jnp.sum(route_score, axis=1, keepdims=True))
    most_rows = min(STRING_COUNT, N_EP * CAP)

    def one_expert(running, pieces):
        expert_index, gate_w, up_w, down_w = pieces
        chosen = route_ids == expert_index
        route_coef = lax.optimization_barrier(jnp.sum(jnp.where(chosen, route_share, 0.0), axis=1))
        is_routed = jnp.any(chosen, axis=1).astype(jnp.int32)
        routed_order = jnp.argsort(1 - is_routed, stable=True)[:most_rows].astype(jnp.int32)
        row_block = jnp.take(moe_in, routed_order, axis=0)
        result = lax.optimization_barrier(swiglu(row_block, gate_w, up_w, down_w).astype(jnp.bfloat16))
        term = route_coef[routed_order][:, None] * result.astype(jnp.float32)
        return (running.at[routed_order].add(term), None)
    routed = lax.scan(one_expert, jnp.zeros((STRING_COUNT, D), jnp.float32), (jnp.arange(EXPERTS, dtype=jnp.int32), w_gate, w_up, w_down))[0]
    shared = swiglu(moe_in, shared_gate, shared_up, shared_down)
    out = (residual + routed + shared).astype(jnp.bfloat16)
    return (out, new_key, new_value)
```

```python
import functools
import math

import jax
import jax.numpy as jnp
from jax import lax
from jax.experimental import pallas as pl
from jax.experimental.pallas import tpu as pltpu
from jax.sharding import PartitionSpec as P

EPSILON = 1e-06
ROUTED_SCALE = 2.5
F32 = jnp.float32
BF16 = jnp.bfloat16


def norm_rows(values, gain_row):
    mean_sq = jnp.mean(values * values, axis=-1, keepdims=True)
    return values * lax.rsqrt(mean_sq + EPSILON) * gain_row.astype(F32)


def dot(left, right):
    return jnp.dot(left, right, preferred_element_type=F32)


def stacked(blocks):
    count, rows, width = blocks.shape
    return blocks.astype(F32).reshape(count * rows, width).astype(BF16)


def layer_kernel(
    n,
    tokens,
    norm_gain,
    head_offset,
    lengths,
    moe_gain,
    route_ids,
    route_score,
    key_shift_h,
    wq_h,
    wk_h,
    wv_h,
    wo_h,
    ck_h,
    cv_h,
    wg_h,
    wu_h,
    wd_h,
    sg_h,
    su_h,
    sd_h,
    out,
    new_key,
    new_value,
    key_shift,
    wq,
    wk,
    wv,
    wo,
    ck,
    cv,
    wg,
    wu,
    wd,
    sg,
    su,
    sd,
    x_send,
    x_recv,
    part_send,
    part_recv,
    q_heads,
    logit_buf,
    att_heads,
    att_all,
    col_send,
    col_recv,
    moe_all,
    res_send,
    res_recv,
    local_sem,
    send_sem,
    recv_sem,
):
    me = lax.axis_index("ep")
    seqs, width = tokens.shape
    shard = width // n
    groups, places = key_shift.shape[1], key_shift.shape[2]
    heads = head_offset.shape[0]
    per_group = heads // groups
    head_dim = ck.shape[2] // groups
    experts_here = wg.shape[0]

    pairs = [
        (wk_h, wk),
        (wv_h, wv),
        (wq_h, wq),
        (ck_h, ck),
        (key_shift_h, key_shift),
        (cv_h, cv),
        (wo_h, wo),
        (sg_h, sg),
        (su_h, su),
        (sd_h, sd),
        (wg_h, wg),
        (wu_h, wu),
        (wd_h, wd),
    ]
    loads = {}
    for place, (source, target) in enumerate(pairs):
        loads[id(target)] = pltpu.make_async_copy(source, target, local_sem.at[place])

    def ready(target):
        loads[id(target)].wait()

    barrier = pltpu.get_barrier_semaphore()

    def greet(step, carry):
        pl.semaphore_signal(
            barrier,
            inc=1,
            device_id={"ep": lax.rem(me + step, n)},
            device_id_type=pl.DeviceIdType.MESH,
        )
        return carry

    lax.fori_loop(1, n, greet, 0)
    for copy in loads.values():
        copy.start()

    def send_all(source_of, target, phase):
        def body(step, carry):
            peer = lax.rem(me + step, n)
            pltpu.make_async_remote_copy(
                src_ref=source_of(peer),
                dst_ref=target.at[me],
                send_sem=send_sem.at[phase],
                recv_sem=recv_sem.at[phase],
                device_id={"ep": peer},
                device_id_type=pl.DeviceIdType.MESH,
            ).start()
            return carry

        lax.fori_loop(1, n, body, 0)

    def wait_blocks(target, sem):
        blocks = target.at[pl.ds(0, n - 1)]
        pltpu.make_async_copy(blocks, blocks, sem).wait()

    residual_in = tokens[...].astype(F32)
    normed = norm_rows(residual_in, norm_gain[...]).astype(BF16)
    for peer in range(n):
        x_send[peer] = normed[:, peer * shard : (peer + 1) * shard]
    x_recv[me] = x_send[me]
    pl.semaphore_wait(barrier, n - 1)
    send_all(lambda peer: x_send.at[peer], x_recv, 0)

    ready(wk)
    new_key[...] = dot(normed, wk[...]).astype(BF16)
    ready(wv)
    new_value[...] = dot(normed, wv[...]).astype(BF16)

    ready(wq)
    wait_blocks(x_recv, recv_sem.at[0])
    part_send[...] = dot(stacked(x_recv[...]), wq[...]).reshape(part_send.shape)
    part_recv[me] = part_send[me]
    send_all(lambda peer: part_send.at[peer], part_recv, 1)

    score = route_score[...]
    share = ROUTED_SCALE * score / jnp.sum(score, axis=1, keepdims=True)
    ids = route_ids[...]

    row = lax.broadcasted_iota(jnp.int32, (heads, 1), 0)
    offset_column = jnp.zeros((heads, 1), F32)
    for head in range(heads):
        offset_column = jnp.where(row == head, head_offset[head], offset_column)
    place_row = lax.broadcasted_iota(jnp.int32, (1, places), 1)
    live_rows = []
    for seq in range(seqs):
        live_rows.append(place_row < lengths[seq])

    wait_blocks(part_recv, recv_sem.at[1])
    queries = jnp.sum(part_recv[...], axis=0).astype(BF16).astype(F32)
    blank = jnp.zeros((seqs, head_dim), F32)
    for head in range(heads):
        pieces = [blank] * groups
        pieces[head // per_group] = queries[:, head * head_dim : (head + 1) * head_dim]
        q_heads[:, head, :] = jnp.concatenate(pieces, axis=1)

    ready(ck)
    ready(key_shift)
    scale = 1.0 / math.sqrt(head_dim)
    for seq in range(seqs):
        product = lax.dot_general(
            q_heads[seq].astype(BF16),
            ck[seq],
            (((1,), (1,)), ((), ())),
            preferred_element_type=F32,
        )
        shift = key_shift[seq]
        shift_rows = jnp.broadcast_to(shift[0:1], (heads, places))
        for group in range(1, groups):
            shift_rows = jnp.where(row // per_group == group, shift[group : group + 1], shift_rows)
        logit_buf[seq] = product * scale + offset_column + shift_rows

    chunk = 128
    later = (
        lax.broadcasted_iota(jnp.int32, (chunk, chunk), 0)
        > lax.broadcasted_iota(jnp.int32, (chunk, chunk), 1)
    ).astype(BF16)
    rows = seqs * heads
    live_count = jnp.concatenate(
        [jnp.full((heads, 1), 0, jnp.int32) + lengths[seq] for seq in range(seqs)], axis=0
    )
    carry = jnp.zeros((rows, 1), F32)
    weights = [None] * (places // chunk)
    for piece in reversed(range(places // chunk)):
        logits = logit_buf[:, :, piece * chunk : (piece + 1) * chunk].reshape(rows, chunk)
        spot = lax.broadcasted_iota(jnp.int32, (rows, chunk), 1) + piece * chunk
        live = spot < live_count
        tail = jnp.log1p(jnp.exp(-jnp.abs(logits)))
        log_take = jnp.minimum(logits, 0.0) - tail
        log_fall = jnp.where(live, jnp.minimum(-logits, 0.0) - tail, 0.0)
        first = log_fall.astype(BF16)
        rest = log_fall - first.astype(F32)
        second = rest.astype(BF16)
        third = (rest - second.astype(F32)).astype(BF16)
        sums = dot(jnp.concatenate([first, second, third], axis=0), later)
        after = (sums[2 * rows :] + sums[rows : 2 * rows]) + sums[:rows] + carry
        weights[piece] = jnp.where(live, jnp.exp(log_take + after), 0.0)
        carry = carry + jnp.sum(log_fall, axis=1, keepdims=True)

    ready(cv)
    for seq in range(seqs):
        own = jnp.concatenate(
            [block[seq * heads : (seq + 1) * heads] for block in weights], axis=1
        ).astype(BF16)
        att_heads[seq] = dot(own, cv[seq])
    pieces = []
    for head in range(heads):
        low = (head // per_group) * head_dim
        pieces.append(att_heads[:, head, :][:, low : low + head_dim])
    att_all[me] = jnp.concatenate(pieces, axis=1).astype(BF16)
    send_all(lambda peer: att_all.at[me], att_all, 2)

    ready(wo)
    wait_blocks(att_all, recv_sem.at[2])
    columns = dot(stacked(att_all[...]), wo[...])
    col_send[...] = columns.reshape(col_send.shape).astype(BF16)
    col_recv[me] = col_send[me]
    send_all(lambda peer: col_send.at[peer], col_recv, 3)
    wait_blocks(col_recv, recv_sem.at[3])
    branch = jnp.concatenate([col_recv[peer].astype(F32) for peer in range(n)], axis=1)
    residual = residual_in + branch
    moe_in = norm_rows(residual, moe_gain[...]).astype(BF16)
    moe_all[me] = moe_in
    send_all(lambda peer: moe_all.at[me], moe_all, 4)

    ready(sg)
    ready(su)
    ready(sd)
    hidden = jax.nn.silu(dot(moe_in, sg[...])) * dot(moe_in, su[...])
    total = residual + dot(hidden.astype(BF16), sd[...])

    ready(wg)
    ready(wu)
    ready(wd)
    wait_blocks(moe_all, recv_sem.at[4])
    moe_rows = stacked(moe_all[...])
    for expert in range(experts_here):
        hidden = jax.nn.silu(dot(moe_rows, wg[expert])) * dot(moe_rows, wu[expert])
        result = dot(hidden.astype(BF16), wd[expert])
        res_send[:, expert] = result.reshape(n, seqs, width).astype(BF16)
    res_recv[me] = res_send[me]
    send_all(lambda peer: res_send.at[peer], res_recv, 5)
    wait_blocks(res_recv, recv_sem.at[5])
    for owner in range(n):
        for expert in range(experts_here):
            chosen = ids == owner * experts_here + expert
            coef = jnp.sum(jnp.where(chosen, share, 0.0), axis=1, keepdims=True)
            total = total + coef * res_recv[owner, expert].astype(F32)
    out[...] = total.astype(BF16)

    wait_blocks(x_send, send_sem.at[0])
    wait_blocks(part_send, send_sem.at[1])
    wait_blocks(att_all, send_sem.at[2])
    wait_blocks(col_send, send_sem.at[3])
    wait_blocks(moe_all, send_sem.at[4])
    wait_blocks(res_send, send_sem.at[5])


def shards(
    tokens,
    norm_gain,
    w_query,
    w_key,
    w_value,
    w_out,
    cache_k,
    cache_v,
    head_offset,
    key_shift,
    lengths,
    moe_gain,
    route_ids,
    route_score,
    w_gate,
    w_up,
    w_down,
    shared_gate,
    shared_up,
    shared_down,
):
    n = lax.axis_size("ep")
    seqs, width = tokens.shape
    query_width = w_query.shape[1]
    shard = w_query.shape[0]
    heads = head_offset.shape[0]
    places, kv_width = cache_k.shape[1:]
    experts_here = w_gate.shape[0]
    vmem = pl.BlockSpec(memory_space=pltpu.VMEM)
    smem = pl.BlockSpec(memory_space=pltpu.SMEM)
    hbm = pl.BlockSpec(memory_space=pl.ANY)
    large = [
        key_shift,
        w_query,
        w_key,
        w_value,
        w_out,
        cache_k,
        cache_v,
        w_gate,
        w_up,
        w_down,
        shared_gate,
        shared_up,
        shared_down,
    ]
    return pl.pallas_call(
        functools.partial(layer_kernel, n),
        out_shape=(
            jax.ShapeDtypeStruct((seqs, width), BF16),
            jax.ShapeDtypeStruct((seqs, w_key.shape[1]), BF16),
            jax.ShapeDtypeStruct((seqs, w_value.shape[1]), BF16),
        ),
        in_specs=[vmem, vmem, smem, smem, vmem, vmem, vmem] + [hbm] * len(large),
        out_specs=(vmem, vmem, vmem),
        scratch_shapes=[pltpu.VMEM(array.shape, array.dtype) for array in large]
        + [
            pltpu.VMEM((n, seqs, shard), BF16),
            pltpu.VMEM((n, seqs, shard), BF16),
            pltpu.VMEM((n, seqs, query_width), F32),
            pltpu.VMEM((n, seqs, query_width), F32),
            pltpu.VMEM((seqs, heads, kv_width), F32),
            pltpu.VMEM((seqs, heads, places), F32),
            pltpu.VMEM((seqs, heads, kv_width), F32),
            pltpu.VMEM((n, seqs, query_width), BF16),
            pltpu.VMEM((n, seqs, w_out.shape[1]), BF16),
            pltpu.VMEM((n, seqs, w_out.shape[1]), BF16),
            pltpu.VMEM((n, seqs, width), BF16),
            pltpu.VMEM((n, experts_here, seqs, width), BF16),
            pltpu.VMEM((n, experts_here, seqs, width), BF16),
            pltpu.SemaphoreType.DMA((len(large),)),
            pltpu.SemaphoreType.DMA((6,)),
            pltpu.SemaphoreType.DMA((6,)),
        ],
        compiler_params=pltpu.CompilerParams(
            collective_id=0, has_side_effects=True, vmem_limit_bytes=60 * 1024 * 1024
        ),
    )(
        tokens,
        norm_gain[None, :],
        head_offset,
        lengths,
        moe_gain[None, :],
        route_ids,
        route_score,
        *large,
    )


def solution(mesh):
    placed = (
        P(("grp", "ep"), None),
        P(),
        P("ep", None),
        P(),
        P(),
        P(None, "ep"),
        P(("grp", "ep"), None, None),
        P(("grp", "ep"), None, None),
        P(),
        P(("grp", "ep"), None, None),
        P(("grp", "ep")),
        P(),
        P(("grp", "ep"), None),
        P(("grp", "ep"), None),
        P("ep", None, None),
        P("ep", None, None),
        P("ep", None, None),
        P(),
        P(),
        P(),
    )
    return jax.shard_map(
        shards,
        mesh=mesh,
        in_specs=placed,
        out_specs=(P(("grp", "ep"), None), P(("grp", "ep"), None), P(("grp", "ep"), None)),
        check_vma=False,
    )
```

```python
import functools
import math

import jax
import jax.numpy as jnp
from jax import lax
from jax.experimental import pallas as pl
from jax.experimental.pallas import tpu as pltpu
from jax.sharding import PartitionSpec as P

EPSILON = 1e-06
ROUTED_SCALE = 2.5
MOE_PARTS = 2
F32 = jnp.float32
BF16 = jnp.bfloat16


def norm_rows(values, gain_row):
    mean_sq = jnp.mean(values * values, axis=-1, keepdims=True)
    return values * lax.rsqrt(mean_sq + EPSILON) * gain_row


def dot(left, right):
    return jnp.dot(left, right, preferred_element_type=F32)


def stacked(blocks):
    count, rows, width = blocks.shape
    return blocks.astype(F32).reshape(count * rows, width).astype(BF16)


def layer_kernel(
    n,
    tokens,
    norm_gain,
    head_offset,
    lengths,
    moe_gain,
    route_ids,
    route_score,
    key_shift_h,
    wq_h,
    wk_h,
    wv_h,
    wo_h,
    ck_h,
    cv_h,
    wg_h,
    wu_h,
    wd_h,
    sg_h,
    su_h,
    sd_h,
    out,
    new_key,
    new_value,
    key_shift,
    wq,
    wk,
    wv,
    wo,
    ck,
    cv,
    wg,
    wu,
    wd,
    sg,
    su,
    sd,
    x_send,
    x_recv,
    part_send,
    part_recv,
    q_heads,
    logit_buf,
    att_heads,
    att_all,
    col_send,
    col_recv,
    coef_all,
    moe_all,
    pair_send,
    pair_recv,
    back_send,
    back_recv,
    local_sem,
    send_sem,
    recv_sem,
    moe_send_sem,
    moe_recv_sem,
    relay_send_sem,
    relay_recv_sem,
    pair_send_sem,
    pair_recv_sem,
):
    me = lax.axis_index("ep")
    chips = n // 2
    chip, core = me // 2, me % 2
    partner = chip * 2 + 1 - core

    def met(step):
        other, bit = chip, 1
        while bit < chips:
            if step & bit:
                other = other + bit * (1 - 2 * (chip // bit % 2))
            bit *= 2
        return other

    def remote(source, target, sent, arrived, device):
        return pltpu.make_async_remote_copy(
            src_ref=source,
            dst_ref=target,
            send_sem=sent,
            recv_sem=arrived,
            device_id={"ep": device},
            device_id_type=pl.DeviceIdType.MESH,
        )

    seqs, width = tokens.shape
    shard = width // n
    groups, places = key_shift.shape[1], key_shift.shape[2]
    heads = head_offset.shape[0]
    per_group = heads // groups
    head_dim = ck.shape[2] // groups
    experts_here = wg.shape[0]

    pairs = [
        (wk_h, wk),
        (wv_h, wv),
        (wq_h, wq),
        (ck_h, ck),
        (key_shift_h, key_shift),
        (cv_h, cv),
        (wo_h, wo),
        (sg_h, sg),
        (su_h, su),
        (sd_h, sd),
        (wg_h, wg),
        (wu_h, wu),
        (wd_h, wd),
    ]
    loads = {}
    for place, (source, target) in enumerate(pairs):
        loads[id(target)] = pltpu.make_async_copy(source, target, local_sem.at[place])

    def ready(target):
        loads[id(target)].wait()

    barrier = pltpu.get_barrier_semaphore()

    def greet(step, carry):
        pl.semaphore_signal(
            barrier,
            inc=1,
            device_id={"ep": lax.rem(me + step, n)},
            device_id_type=pl.DeviceIdType.MESH,
        )
        return carry

    lax.fori_loop(1, n, greet, 0)
    for copy in loads.values():
        copy.start()

    def send_all(source_of, target, phase):
        def body(step, carry):
            peer = lax.rem(me + step, n)
            remote(
                source_of(peer), target.at[me], send_sem.at[phase], recv_sem.at[phase], peer
            ).start()
            return carry

        lax.fori_loop(1, n, body, 0)

    def wait_blocks(target, sem):
        blocks = target.at[pl.ds(0, n - 1)]
        pltpu.make_async_copy(blocks, blocks, sem).wait()

    residual_in = tokens[...].astype(F32)
    normed = norm_rows(residual_in, norm_gain[...].astype(F32).reshape(1, width)).astype(BF16)
    for peer in range(n):
        x_send[peer] = normed[:, peer * shard : (peer + 1) * shard]
    x_recv[me] = x_send[me]
    pl.semaphore_wait(barrier, n - 1)
    send_all(lambda peer: x_send.at[peer], x_recv, 0)

    score = route_score[...]
    share = ROUTED_SCALE * score / jnp.sum(score, axis=1, keepdims=True)
    ids = route_ids[...]
    expert_lane = lax.broadcasted_iota(jnp.int32, coef_all.shape[1:], 1)
    table = jnp.zeros(coef_all.shape[1:], F32)
    for pick in range(ids.shape[1]):
        table = table + jnp.where(ids[:, pick : pick + 1] == expert_lane, share[:, pick : pick + 1], 0.0)
    coef_all[me] = table
    send_all(lambda peer: coef_all.at[me], coef_all, 4)

    ready(wk)
    new_key[...] = dot(normed, wk[...]).astype(BF16)
    ready(wv)
    new_value[...] = dot(normed, wv[...]).astype(BF16)

    ready(wq)
    wait_blocks(x_recv, recv_sem.at[0])
    part_send[...] = dot(stacked(x_recv[...]), wq[...]).reshape(part_send.shape).astype(BF16)
    part_recv[me] = part_send[me]
    send_all(lambda peer: part_send.at[peer], part_recv, 1)

    row = lax.broadcasted_iota(jnp.int32, (heads, 1), 0)
    offset_column = jnp.zeros((heads, 1), F32)
    for head in range(heads):
        offset_column = jnp.where(row == head, head_offset[head], offset_column)
    place_row = lax.broadcasted_iota(jnp.int32, (1, places), 1)
    live_rows = []
    for seq in range(seqs):
        live_rows.append(place_row < lengths[seq])

    wait_blocks(part_recv, recv_sem.at[1])
    queries = jnp.sum(part_recv[...].astype(F32), axis=0).astype(BF16).astype(F32)
    blank = jnp.zeros((seqs, head_dim), F32)
    for head in range(heads):
        pieces = [blank] * groups
        pieces[head // per_group] = queries[:, head * head_dim : (head + 1) * head_dim]
        q_heads[:, head, :] = jnp.concatenate(pieces, axis=1)

    ready(ck)
    ready(key_shift)
    scale = 1.0 / math.sqrt(head_dim)
    for seq in range(seqs):
        product = lax.dot_general(
            q_heads[seq].astype(BF16),
            ck[seq],
            (((1,), (1,)), ((), ())),
            preferred_element_type=F32,
        )
        shift = key_shift[seq]
        shift_rows = jnp.broadcast_to(shift[0:1], (heads, places))
        for group in range(1, groups):
            shift_rows = jnp.where(row // per_group == group, shift[group : group + 1], shift_rows)
        logit_buf[seq] = product * scale + offset_column + shift_rows

    chunk = 128
    later = (
        lax.broadcasted_iota(jnp.int32, (chunk, chunk), 0)
        > lax.broadcasted_iota(jnp.int32, (chunk, chunk), 1)
    ).astype(BF16)
    rows = seqs * heads
    live_count = jnp.concatenate(
        [jnp.full((heads, 1), 0, jnp.int32) + lengths[seq] for seq in range(seqs)], axis=0
    )
    carry = jnp.zeros((rows, 1), F32)
    weights = [None] * (places // chunk)
    for piece in reversed(range(places // chunk)):
        logits = logit_buf[:, :, piece * chunk : (piece + 1) * chunk].reshape(rows, chunk)
        spot = lax.broadcasted_iota(jnp.int32, (rows, chunk), 1) + piece * chunk
        live = spot < live_count
        tail = jnp.log1p(jnp.exp(-jnp.abs(logits)))
        log_take = jnp.minimum(logits, 0.0) - tail
        log_fall = jnp.where(live, jnp.minimum(-logits, 0.0) - tail, 0.0)
        first = log_fall.astype(BF16)
        rest = log_fall - first.astype(F32)
        second = rest.astype(BF16)
        third = (rest - second.astype(F32)).astype(BF16)
        sums = dot(jnp.concatenate([first, second, third], axis=0), later)
        after = (sums[2 * rows :] + sums[rows : 2 * rows]) + sums[:rows] + carry
        weights[piece] = jnp.where(live, jnp.exp(log_take + after), 0.0)
        carry = carry + jnp.sum(log_fall, axis=1, keepdims=True)

    ready(cv)
    for seq in range(seqs):
        own = jnp.concatenate(
            [block[seq * heads : (seq + 1) * heads] for block in weights], axis=1
        ).astype(BF16)
        att_heads[seq] = dot(own, cv[seq])
    pieces = []
    for head in range(heads):
        low = (head // per_group) * head_dim
        pieces.append(att_heads[:, head, :][:, low : low + head_dim])
    att_all[me] = jnp.concatenate(pieces, axis=1).astype(BF16)
    send_all(lambda peer: att_all.at[me], att_all, 2)

    ready(wo)
    wait_blocks(att_all, recv_sem.at[2])
    columns = dot(stacked(att_all[...]), wo[...])
    col_send[...] = columns.reshape(col_send.shape).astype(BF16)
    col_recv[me] = col_send[me]
    send_all(lambda peer: col_send.at[peer], col_recv, 3)
    wait_blocks(col_recv, recv_sem.at[3])
    branch = jnp.concatenate([col_recv[peer].astype(F32) for peer in range(n)], axis=1)
    residual = residual_in + branch
    moe_in = norm_rows(residual, moe_gain[...].astype(F32).reshape(1, width)).astype(BF16)
    moe_all[me] = moe_in
    relays = [remote(moe_all.at[me], moe_all.at[me], relay_send_sem.at[0], relay_recv_sem.at[0], partner)]
    relays[0].start()
    spread = [None]
    for step in range(1, chips):
        copy = remote(
            moe_all.at[me],
            moe_all.at[me],
            moe_send_sem.at[step],
            moe_recv_sem.at[step],
            met(step) * 2 + core,
        )
        copy.start()
        spread.append(copy)

    ready(sg)
    ready(su)
    ready(sd)
    hidden = jax.nn.silu(dot(moe_in, sg[...])) * dot(moe_in, su[...])
    total = residual + dot(hidden.astype(BF16), sd[...])

    wait_blocks(coef_all, recv_sem.at[4])
    ready(wg)
    ready(wu)
    ready(wd)
    parts = pair_send.shape[0]
    group = chips // parts
    backs = []
    for part in range(parts):
        steps = range(part * group, (part + 1) * group)
        for step in steps:
            if step > 0:
                spread[step].wait_recv()
                held = moe_all.at[met(step) * 2 + core]
                copy = remote(held, held, relay_send_sem.at[step], relay_recv_sem.at[step], partner)
                copy.start()
                relays.append(copy)
        for step in steps:
            relays[step].wait_recv()
        owners = [met(step) * 2 + core for step in steps]
        owners += [met(step) * 2 + 1 - core for step in steps]
        moe_rows = jnp.concatenate([moe_all[owner].astype(F32) for owner in owners], axis=0).astype(BF16)
        coefs = jnp.concatenate([coef_all[owner] for owner in owners], axis=0)
        lane = lax.broadcasted_iota(jnp.int32, coefs.shape, 1)
        mixed = None
        for expert in range(experts_here):
            hidden = jax.nn.silu(dot(moe_rows, wg[expert])) * dot(moe_rows, wu[expert])
            result = dot(hidden.astype(BF16), wd[expert]).astype(BF16).astype(F32)
            mine = lane == me * experts_here + expert
            term = jnp.sum(jnp.where(mine, coefs, 0.0), axis=1, keepdims=True) * result
            mixed = term if mixed is None else mixed + term
        mixed = mixed.reshape(2, group, seqs, width)
        pair_send[part] = mixed[1].astype(BF16)
        copy = remote(
            pair_send.at[part],
            pair_recv.at[part],
            pair_send_sem.at[part],
            pair_recv_sem.at[part],
            partner,
        )
        copy.start()
        copy.wait_recv()
        both = mixed[0] + pair_recv[part].astype(F32)
        for place, step in enumerate(steps):
            if step == 0:
                total = total + both[place]
                continue
            back_send[step - 1] = both[place].astype(BF16)
            remote(
                back_send.at[step - 1],
                back_recv.at[step - 1],
                send_sem.at[5],
                recv_sem.at[5],
                met(step) * 2 + core,
            ).start()
        backs.append(copy)
    pltpu.make_async_copy(back_recv, back_recv, recv_sem.at[5]).wait()
    for step in range(chips - 1):
        total = total + back_recv[step].astype(F32)
    out[...] = total.astype(BF16)

    wait_blocks(x_send, send_sem.at[0])
    wait_blocks(part_send, send_sem.at[1])
    wait_blocks(att_all, send_sem.at[2])
    wait_blocks(col_send, send_sem.at[3])
    wait_blocks(coef_all, send_sem.at[4])
    pltpu.make_async_copy(back_send, back_send, send_sem.at[5]).wait()
    for copy in spread[1:] + relays + backs:
        copy.wait_send()


def hand_on_kernel(*refs):
    for source, target in zip(refs[: len(refs) // 2], refs[len(refs) // 2 :]):
        target[...] = source[...]


def shards(
    tokens,
    norm_gain,
    w_query,
    w_key,
    w_value,
    w_out,
    cache_k,
    cache_v,
    head_offset,
    key_shift,
    lengths,
    moe_gain,
    route_ids,
    route_score,
    w_gate,
    w_up,
    w_down,
    shared_gate,
    shared_up,
    shared_down,
):
    n = lax.axis_size("ep")
    seqs, width = tokens.shape
    query_width = w_query.shape[1]
    shard = w_query.shape[0]
    heads = head_offset.shape[0]
    places, kv_width = cache_k.shape[1:]
    experts_here = w_gate.shape[0]
    vmem = pl.BlockSpec(memory_space=pltpu.VMEM)
    smem = pl.BlockSpec(memory_space=pltpu.SMEM)
    hbm = pl.BlockSpec(memory_space=pl.ANY)
    large = [
        key_shift,
        w_query,
        w_key,
        w_value,
        w_out,
        cache_k,
        cache_v,
        w_gate,
        w_up,
        w_down,
        shared_gate,
        shared_up,
        shared_down,
    ]
    chips = n // 2
    parts = min(MOE_PARTS, chips)
    out_shape = (
        jax.ShapeDtypeStruct((seqs, width), BF16),
        jax.ShapeDtypeStruct((seqs, w_key.shape[1]), BF16),
        jax.ShapeDtypeStruct((seqs, w_value.shape[1]), BF16),
    )
    results = pl.pallas_call(
        functools.partial(layer_kernel, n),
        out_shape=out_shape,
        in_specs=[vmem, vmem, smem, smem, vmem, vmem, vmem] + [hbm] * len(large),
        out_specs=(vmem, vmem, vmem),
        scratch_shapes=[pltpu.VMEM(array.shape, array.dtype) for array in large]
        + [
            pltpu.VMEM((n, seqs, shard), BF16),
            pltpu.VMEM((n, seqs, shard), BF16),
            pltpu.VMEM((n, seqs, query_width), BF16),
            pltpu.VMEM((n, seqs, query_width), BF16),
            pltpu.VMEM((seqs, heads, kv_width), F32),
            pltpu.VMEM((seqs, heads, places), F32),
            pltpu.VMEM((seqs, heads, kv_width), F32),
            pltpu.VMEM((n, seqs, query_width), BF16),
            pltpu.VMEM((n, seqs, w_out.shape[1]), BF16),
            pltpu.VMEM((n, seqs, w_out.shape[1]), BF16),
            pltpu.VMEM((n, seqs, n * experts_here), F32),
            pltpu.VMEM((n, seqs, width), BF16),
            pltpu.VMEM((parts, chips // parts, seqs, width), BF16),
            pltpu.VMEM((parts, chips // parts, seqs, width), BF16),
            pltpu.VMEM((chips - 1, seqs, width), BF16),
            pltpu.VMEM((chips - 1, seqs, width), BF16),
            pltpu.SemaphoreType.DMA((len(large),)),
            pltpu.SemaphoreType.DMA((6,)),
            pltpu.SemaphoreType.DMA((6,)),
            pltpu.SemaphoreType.DMA((chips,)),
            pltpu.SemaphoreType.DMA((chips,)),
            pltpu.SemaphoreType.DMA((chips,)),
            pltpu.SemaphoreType.DMA((chips,)),
            pltpu.SemaphoreType.DMA((parts,)),
            pltpu.SemaphoreType.DMA((parts,)),
        ],
        compiler_params=pltpu.CompilerParams(
            collective_id=0, has_side_effects=True, vmem_limit_bytes=60 * 1024 * 1024
        ),
    )(
        tokens,
        norm_gain,
        head_offset,
        lengths,
        moe_gain,
        route_ids,
        route_score,
        *large,
    )
    return pl.pallas_call(
        hand_on_kernel,
        out_shape=out_shape,
        in_specs=[vmem] * 3,
        out_specs=(vmem, vmem, vmem),
    )(*results)


def solution(mesh):
    placed = (
        P(("grp", "ep"), None),
        P(),
        P("ep", None),
        P(),
        P(),
        P(None, "ep"),
        P(("grp", "ep"), None, None),
        P(("grp", "ep"), None, None),
        P(),
        P(("grp", "ep"), None, None),
        P(("grp", "ep")),
        P(),
        P(("grp", "ep"), None),
        P(("grp", "ep"), None),
        P("ep", None, None),
        P("ep", None, None),
        P("ep", None, None),
        P(),
        P(),
        P(),
    )
    return jax.shard_map(
        shards,
        mesh=mesh,
        in_specs=placed,
        out_specs=(P(("grp", "ep"), None), P(("grp", "ep"), None), P(("grp", "ep"), None)),
        check_vma=False,
    )
```

```python
import functools
import math

import jax
import jax.numpy as jnp
from jax import lax
from jax.experimental import pallas as pl
from jax.experimental.pallas import tpu as pltpu
from jax.sharding import PartitionSpec as P

EPSILON = 1e-06
ROUTED_SCALE = 2.5
MOE_PARTS = 4
NEAR = 4
F32 = jnp.float32
BF16 = jnp.bfloat16


def norm_rows(values, gain_row):
    mean_sq = jnp.mean(values * values, axis=-1, keepdims=True)
    return values * lax.rsqrt(mean_sq + EPSILON) * gain_row


def dot(left, right):
    return jnp.dot(left, right, preferred_element_type=F32)


def stacked(blocks):
    count, rows, width = blocks.shape
    return blocks.astype(F32).reshape(count * rows, width).astype(BF16)


def layer_kernel(
    n,
    tokens_h,
    norm_gain_h,
    head_offset_h,
    lengths_h,
    moe_gain_h,
    route_ids_h,
    route_score_h,
    key_shift_h,
    wq_h,
    wk_h,
    wv_h,
    wo_h,
    ck_h,
    cv_h,
    wg_h,
    wu_h,
    wd_h,
    sg_h,
    su_h,
    sd_h,
    out,
    new_key,
    new_value,
    tokens,
    norm_gain,
    head_offset,
    lengths,
    moe_gain,
    route_ids,
    route_score,
    key_shift,
    wq,
    wk,
    wv,
    wo_all,
    ck,
    cv,
    wg,
    wu,
    wd,
    sg,
    su,
    sd,
    x_send,
    x_recv,
    part_send,
    part_recv,
    q_heads,
    logit_buf,
    att_heads,
    att_all,
    col_send,
    col_recv,
    coef_all,
    moe_all,
    pair_send,
    pair_recv,
    back_send,
    back_recv,
    local_sem,
    send_sem,
    recv_sem,
    moe_send_sem,
    moe_recv_sem,
    relay_send_sem,
    relay_recv_sem,
    pair_send_sem,
    pair_recv_sem,
    chain_send_sem,
    chain_recv_sem,
):
    me = lax.axis_index("ep")
    chips = n // 2
    chip, core = me // 2, me % 2
    partner = chip * 2 + 1 - core

    def met(step):
        other, bit = chip, 1
        while bit < chips:
            if step & bit:
                other = other + bit * (1 - 2 * (chip // bit % 2))
            bit *= 2
        return other

    def remote(source, target, sent, arrived, device):
        return pltpu.make_async_remote_copy(
            src_ref=source,
            dst_ref=target,
            send_sem=sent,
            recv_sem=arrived,
            device_id={"ep": device},
            device_id_type=pl.DeviceIdType.MESH,
        )

    seqs, width = tokens.shape
    shard = width // n
    groups, places = key_shift.shape[1], key_shift.shape[2]
    heads = head_offset.shape[0]
    per_group = heads // groups
    head_dim = ck.shape[2] // groups
    experts_here = wg.shape[0]

    near = NEAR
    tiers = n // near
    tier, seat = me // near, me % near
    wo = wo_all.at[tier]

    pairs = [
        (tokens_h, tokens),
        (norm_gain_h, norm_gain),
        (wo_h, wo),
        (wk_h, wk),
        (wv_h, wv),
        (wq_h, wq),
        (route_ids_h, route_ids),
        (route_score_h, route_score),
        (head_offset_h, head_offset),
        (lengths_h, lengths),
        (moe_gain_h, moe_gain),
        (ck_h, ck),
        (key_shift_h, key_shift),
        (cv_h, cv),
        (sg_h, sg),
        (su_h, su),
        (sd_h, sd),
        (wg_h, wg),
        (wu_h, wu),
        (wd_h, wd),
    ]
    loads = {}
    for place, (source, target) in enumerate(pairs):
        loads[id(target)] = pltpu.make_async_copy(source, target, local_sem.at[place])

    def ready(target):
        loads[id(target)].wait()

    barrier = pltpu.get_barrier_semaphore()

    def greet(step, carry):
        pl.semaphore_signal(
            barrier,
            inc=1,
            device_id={"ep": lax.rem(me + step, n)},
            device_id_type=pl.DeviceIdType.MESH,
        )
        return carry

    lax.fori_loop(1, n, greet, 0)
    for copy in loads.values():
        copy.start()

    def send_all(source_of, target, phase):
        def body(step, carry):
            peer = lax.rem(me + step, n)
            remote(
                source_of(peer), target.at[me], send_sem.at[phase], recv_sem.at[phase], peer
            ).start()
            return carry

        lax.fori_loop(1, n, body, 0)

    def send_near(source_of, target, phase):
        for step in range(1, near):
            place = (seat + step) % near
            remote(
                source_of(place),
                target.at[seat],
                send_sem.at[phase],
                recv_sem.at[phase],
                tier * near + place,
            ).start()

    def chain(step):
        below, above = tier - step + 1, tier + step - 1
        up = ((tier < tiers - 1) & (below >= 0), below, me + near, 0)
        down = ((tier > 0) & (above < tiers), above, me - near, 1)
        return [
            (
                active,
                lambda held=held, device=device, way=way: remote(
                    wo_all.at[held],
                    wo_all.at[held],
                    chain_send_sem.at[way, step],
                    chain_recv_sem.at[way, step],
                    device,
                ),
            )
            for active, held, device, way in (up, down)
        ]

    def chain_send(step):
        for active, copy in chain(step):
            pl.when(active)(lambda copy=copy: copy().start())

    def chain_sent(step):
        for active, copy in chain(step):
            pl.when(active)(lambda copy=copy: copy().wait_send())

    def chain_wait(step):
        for active, held, way in ((tier >= step, tier - step, 0), (tier + step < tiers, tier + step, 1)):

            def arrived(held=held, way=way):
                block = wo_all.at[held]
                pltpu.make_async_copy(block, block, chain_recv_sem.at[way, step]).wait()

            pl.when(active)(arrived)

    def wait_blocks(target, sem):
        blocks = target.at[pl.ds(0, target.shape[0] - 1)]
        pltpu.make_async_copy(blocks, blocks, sem).wait()

    ready(tokens)
    ready(norm_gain)
    residual_in = tokens[...].astype(F32)
    normed = norm_rows(residual_in, norm_gain[...].astype(F32).reshape(1, width)).astype(BF16)
    for peer in range(n):
        x_send[peer] = normed[:, peer * shard : (peer + 1) * shard]
    x_recv[me] = x_send[me]
    pl.semaphore_wait(barrier, n - 1)
    send_all(lambda peer: x_send.at[peer], x_recv, 0)

    ready(wo)
    chain_send(1)

    ready(route_ids)
    ready(route_score)
    score = route_score[...]
    share = ROUTED_SCALE * score / jnp.sum(score, axis=1, keepdims=True)
    ids = route_ids[...]
    expert_lane = lax.broadcasted_iota(jnp.int32, coef_all.shape[1:], 1)
    table = jnp.zeros(coef_all.shape[1:], F32)
    for pick in range(ids.shape[1]):
        table = table + jnp.where(ids[:, pick : pick + 1] == expert_lane, share[:, pick : pick + 1], 0.0)
    coef_all[me] = table

    ready(wk)
    new_key[...] = dot(normed, wk[...]).astype(BF16)
    ready(wv)
    new_value[...] = dot(normed, wv[...]).astype(BF16)

    ready(wq)
    wait_blocks(x_recv, recv_sem.at[0])
    part_send[...] = dot(stacked(x_recv[...]), wq[...]).reshape(part_send.shape).astype(BF16)
    part_recv[me] = part_send[me]
    send_all(lambda peer: part_send.at[peer], part_recv, 1)

    ready(head_offset)
    ready(lengths)
    ready(moe_gain)
    row = lax.broadcasted_iota(jnp.int32, (heads, 1), 0)
    offset_column = jnp.zeros((heads, 1), F32)
    for head in range(heads):
        offset_column = jnp.where(row == head, head_offset[head], offset_column)
    place_row = lax.broadcasted_iota(jnp.int32, (1, places), 1)
    live_rows = []
    for seq in range(seqs):
        live_rows.append(place_row < lengths[seq])

    if tiers > 1:
        chain_wait(1)
        chain_send(2)
    wait_blocks(part_recv, recv_sem.at[1])
    if tiers > 2:
        chain_wait(2)
        chain_send(3)
    send_all(lambda peer: coef_all.at[me], coef_all, 4)
    queries = jnp.sum(part_recv[...].astype(F32), axis=0).astype(BF16).astype(F32)
    blank = jnp.zeros((seqs, head_dim), F32)
    for head in range(heads):
        pieces = [blank] * groups
        pieces[head // per_group] = queries[:, head * head_dim : (head + 1) * head_dim]
        q_heads[:, head, :] = jnp.concatenate(pieces, axis=1)

    ready(ck)
    ready(key_shift)
    scale = 1.0 / math.sqrt(head_dim)
    for seq in range(seqs):
        product = lax.dot_general(
            q_heads[seq].astype(BF16),
            ck[seq],
            (((1,), (1,)), ((), ())),
            preferred_element_type=F32,
        )
        shift = key_shift[seq]
        shift_rows = jnp.broadcast_to(shift[0:1], (heads, places))
        for group in range(1, groups):
            shift_rows = jnp.where(row // per_group == group, shift[group : group + 1], shift_rows)
        logit_buf[seq] = product * scale + offset_column + shift_rows

    chunk = 128
    later = (
        lax.broadcasted_iota(jnp.int32, (chunk, chunk), 0)
        > lax.broadcasted_iota(jnp.int32, (chunk, chunk), 1)
    ).astype(BF16)
    rows = seqs * heads
    live_count = jnp.concatenate(
        [jnp.full((heads, 1), 0, jnp.int32) + lengths[seq] for seq in range(seqs)], axis=0
    )
    carry = jnp.zeros((rows, 1), F32)
    weights = [None] * (places // chunk)
    for piece in reversed(range(places // chunk)):
        logits = logit_buf[:, :, piece * chunk : (piece + 1) * chunk].reshape(rows, chunk)
        spot = lax.broadcasted_iota(jnp.int32, (rows, chunk), 1) + piece * chunk
        live = spot < live_count
        tail = jnp.log1p(jnp.exp(-jnp.abs(logits)))
        log_take = jnp.minimum(logits, 0.0) - tail
        log_fall = jnp.where(live, jnp.minimum(-logits, 0.0) - tail, 0.0)
        first = log_fall.astype(BF16)
        rest = log_fall - first.astype(F32)
        second = rest.astype(BF16)
        third = (rest - second.astype(F32)).astype(BF16)
        sums = dot(jnp.concatenate([first, second, third], axis=0), later)
        after = (sums[2 * rows :] + sums[rows : 2 * rows]) + sums[:rows] + carry
        weights[piece] = jnp.where(live, jnp.exp(log_take + after), 0.0)
        carry = carry + jnp.sum(log_fall, axis=1, keepdims=True)

    ready(cv)
    for seq in range(seqs):
        own = jnp.concatenate(
            [block[seq * heads : (seq + 1) * heads] for block in weights], axis=1
        ).astype(BF16)
        att_heads[seq] = dot(own, cv[seq])
    pieces = []
    for head in range(heads):
        low = (head // per_group) * head_dim
        pieces.append(att_heads[:, head, :][:, low : low + head_dim])
    att_all[seat] = jnp.concatenate(pieces, axis=1).astype(BF16)
    send_near(lambda place: att_all.at[seat], att_all, 2)

    for step in range(3, tiers):
        chain_wait(step)
        chain_send(step + 1)
    wait_blocks(att_all, recv_sem.at[2])
    att_rows = stacked(att_all[...])
    for other in range(tiers):
        columns = dot(att_rows, wo_all[other]).astype(BF16)
        col_send[:, other] = columns.astype(F32).reshape(near, seqs, shard).astype(BF16)
    col_recv[seat] = col_send[seat]
    send_near(lambda place: col_send.at[place], col_recv, 3)
    wait_blocks(col_recv, recv_sem.at[3])
    branch = jnp.concatenate(
        [col_recv[owner % near, owner // near].astype(F32) for owner in range(n)], axis=1
    )
    residual = residual_in + branch
    moe_in = norm_rows(residual, moe_gain[...].astype(F32).reshape(1, width)).astype(BF16)
    moe_all[me] = moe_in
    relays = [remote(moe_all.at[me], moe_all.at[me], relay_send_sem.at[0], relay_recv_sem.at[0], partner)]
    relays[0].start()
    spread = [None]
    for step in range(1, chips):
        copy = remote(
            moe_all.at[me],
            moe_all.at[me],
            moe_send_sem.at[step],
            moe_recv_sem.at[step],
            met(step) * 2 + core,
        )
        copy.start()
        spread.append(copy)

    ready(sg)
    ready(su)
    ready(sd)
    hidden = jax.nn.silu(dot(moe_in, sg[...])) * dot(moe_in, su[...])
    total = residual + dot(hidden.astype(BF16), sd[...])

    wait_blocks(coef_all, recv_sem.at[4])
    ready(wg)
    ready(wu)
    ready(wd)
    parts = pair_send.shape[0]
    group = chips // parts
    backs = []
    for part in range(parts):
        steps = range(part * group, (part + 1) * group)
        for step in steps:
            if step > 0:
                spread[step].wait_recv()
                held = moe_all.at[met(step) * 2 + core]
                copy = remote(held, held, relay_send_sem.at[step], relay_recv_sem.at[step], partner)
                copy.start()
                relays.append(copy)
        for step in steps:
            relays[step].wait_recv()
        owners = [met(step) * 2 + core for step in steps]
        owners += [met(step) * 2 + 1 - core for step in steps]
        moe_rows = jnp.concatenate([moe_all[owner].astype(F32) for owner in owners], axis=0).astype(BF16)
        coefs = jnp.concatenate([coef_all[owner] for owner in owners], axis=0)
        lane = lax.broadcasted_iota(jnp.int32, coefs.shape, 1)
        mixed = None
        for expert in range(experts_here):
            hidden = jax.nn.silu(dot(moe_rows, wg[expert])) * dot(moe_rows, wu[expert])
            result = dot(hidden.astype(BF16), wd[expert]).astype(BF16).astype(F32)
            mine = lane == me * experts_here + expert
            term = jnp.sum(jnp.where(mine, coefs, 0.0), axis=1, keepdims=True) * result
            mixed = term if mixed is None else mixed + term
        mixed = mixed.reshape(2, group, seqs, width)
        pair_send[part] = mixed[1].astype(BF16)
        copy = remote(
            pair_send.at[part],
            pair_recv.at[part],
            pair_send_sem.at[part],
            pair_recv_sem.at[part],
            partner,
        )
        copy.start()
        copy.wait_recv()
        both = mixed[0] + pair_recv[part].astype(F32)
        for place, step in enumerate(steps):
            if step == 0:
                total = total + both[place]
                continue
            back_send[step - 1] = both[place].astype(BF16)
            remote(
                back_send.at[step - 1],
                back_recv.at[step - 1],
                send_sem.at[5],
                recv_sem.at[5],
                met(step) * 2 + core,
            ).start()
        backs.append(copy)
    pltpu.make_async_copy(back_recv, back_recv, recv_sem.at[5]).wait()
    for step in range(chips - 1):
        total = total + back_recv[step].astype(F32)
    out[...] = total.astype(BF16)

    wait_blocks(x_send, send_sem.at[0])
    wait_blocks(part_send, send_sem.at[1])
    wait_blocks(att_all, send_sem.at[2])
    wait_blocks(col_send, send_sem.at[3])
    wait_blocks(coef_all, send_sem.at[4])
    for step in range(1, tiers):
        chain_sent(step)
    pltpu.make_async_copy(back_send, back_send, send_sem.at[5]).wait()
    for copy in spread[1:] + relays + backs:
        copy.wait_send()


def hand_on_kernel(*refs):
    for source, target in zip(refs[: len(refs) // 2], refs[len(refs) // 2 :]):
        target[...] = source[...]


def shards(
    tokens,
    norm_gain,
    w_query,
    w_key,
    w_value,
    w_out,
    cache_k,
    cache_v,
    head_offset,
    key_shift,
    lengths,
    moe_gain,
    route_ids,
    route_score,
    w_gate,
    w_up,
    w_down,
    shared_gate,
    shared_up,
    shared_down,
):
    n = lax.axis_size("ep")
    seqs, width = tokens.shape
    query_width = w_query.shape[1]
    shard = w_query.shape[0]
    heads = head_offset.shape[0]
    places, kv_width = cache_k.shape[1:]
    experts_here = w_gate.shape[0]
    vmem = pl.BlockSpec(memory_space=pltpu.VMEM)
    hbm = pl.BlockSpec(memory_space=pl.ANY)
    tiers = n // NEAR
    scalars = [head_offset, lengths]
    arrays = [
        tokens,
        norm_gain,
        head_offset,
        lengths,
        moe_gain,
        route_ids,
        route_score,
        key_shift,
        w_query,
        w_key,
        w_value,
        w_out,
        cache_k,
        cache_v,
        w_gate,
        w_up,
        w_down,
        shared_gate,
        shared_up,
        shared_down,
    ]
    held = []
    for array in arrays:
        space = pltpu.SMEM if any(array is scalar for scalar in scalars) else pltpu.VMEM
        shape = (tiers, *array.shape) if array is w_out else array.shape
        held.append(space(shape, array.dtype))
    chips = n // 2
    parts = min(MOE_PARTS, chips)
    out_shape = (
        jax.ShapeDtypeStruct((seqs, width), BF16),
        jax.ShapeDtypeStruct((seqs, w_key.shape[1]), BF16),
        jax.ShapeDtypeStruct((seqs, w_value.shape[1]), BF16),
    )
    results = pl.pallas_call(
        functools.partial(layer_kernel, n),
        out_shape=out_shape,
        in_specs=[hbm] * len(arrays),
        out_specs=(vmem, vmem, vmem),
        scratch_shapes=held
        + [
            pltpu.VMEM((n, seqs, shard), BF16),
            pltpu.VMEM((n, seqs, shard), BF16),
            pltpu.VMEM((n, seqs, query_width), BF16),
            pltpu.VMEM((n, seqs, query_width), BF16),
            pltpu.VMEM((seqs, heads, kv_width), F32),
            pltpu.VMEM((seqs, heads, places), F32),
            pltpu.VMEM((seqs, heads, kv_width), F32),
            pltpu.VMEM((NEAR, seqs, query_width), BF16),
            pltpu.VMEM((NEAR, tiers, seqs, w_out.shape[1]), BF16),
            pltpu.VMEM((NEAR, tiers, seqs, w_out.shape[1]), BF16),
            pltpu.VMEM((n, seqs, n * experts_here), F32),
            pltpu.VMEM((n, seqs, width), BF16),
            pltpu.VMEM((parts, chips // parts, seqs, width), BF16),
            pltpu.VMEM((parts, chips // parts, seqs, width), BF16),
            pltpu.VMEM((chips - 1, seqs, width), BF16),
            pltpu.VMEM((chips - 1, seqs, width), BF16),
            pltpu.SemaphoreType.DMA((len(arrays),)),
            pltpu.SemaphoreType.DMA((6,)),
            pltpu.SemaphoreType.DMA((6,)),
            pltpu.SemaphoreType.DMA((chips,)),
            pltpu.SemaphoreType.DMA((chips,)),
            pltpu.SemaphoreType.DMA((chips,)),
            pltpu.SemaphoreType.DMA((chips,)),
            pltpu.SemaphoreType.DMA((parts,)),
            pltpu.SemaphoreType.DMA((parts,)),
            pltpu.SemaphoreType.DMA((2, tiers + 1)),
            pltpu.SemaphoreType.DMA((2, tiers + 1)),
        ],
        compiler_params=pltpu.CompilerParams(
            collective_id=0, has_side_effects=True, vmem_limit_bytes=60 * 1024 * 1024
        ),
    )(*arrays)
    return pl.pallas_call(
        hand_on_kernel,
        out_shape=out_shape,
        in_specs=[vmem] * 3,
        out_specs=(vmem, vmem, vmem),
    )(*results)


def solution(mesh):
    placed = (
        P(("grp", "ep"), None),
        P(),
        P("ep", None),
        P(),
        P(),
        P(None, "ep"),
        P(("grp", "ep"), None, None),
        P(("grp", "ep"), None, None),
        P(),
        P(("grp", "ep"), None, None),
        P(("grp", "ep")),
        P(),
        P(("grp", "ep"), None),
        P(("grp", "ep"), None),
        P("ep", None, None),
        P("ep", None, None),
        P("ep", None, None),
        P(),
        P(),
        P(),
    )
    return jax.shard_map(
        shards,
        mesh=mesh,
        in_specs=placed,
        out_specs=(P(("grp", "ep"), None), P(("grp", "ep"), None), P(("grp", "ep"), None)),
        check_vma=False,
    )
```

```python
import functools
import math

import jax
import jax.numpy as jnp
from jax import lax
from jax.experimental import pallas as pl
from jax.experimental.pallas import tpu as pltpu
from jax.sharding import PartitionSpec as P

EPSILON = 1e-06
ROUTED_SCALE = 2.5
MOE_PARTS = 4
NEAR = 4
F32 = jnp.float32
BF16 = jnp.bfloat16


def norm_rows(values, gain_row):
    mean_sq = jnp.mean(values * values, axis=-1, keepdims=True)
    return values * lax.rsqrt(mean_sq + EPSILON) * gain_row


def dot(left, right):
    return jnp.dot(left, right, preferred_element_type=F32)


def stacked(blocks):
    count, rows, width = blocks.shape
    return blocks.astype(F32).reshape(count * rows, width).astype(BF16)


def layer_kernel(
    n,
    tokens_h,
    norm_gain_h,
    head_offset_h,
    lengths_h,
    moe_gain_h,
    route_ids_h,
    route_score_h,
    key_shift_h,
    wq_h,
    wk_h,
    wv_h,
    wo_h,
    ck_h,
    cv_h,
    wg_h,
    wu_h,
    wd_h,
    sg_h,
    su_h,
    sd_h,
    out,
    new_key,
    new_value,
    tokens,
    norm_gain,
    head_offset,
    lengths,
    moe_gain,
    route_ids,
    route_score,
    key_shift,
    wq,
    wk,
    wv,
    wo_all,
    ck,
    cv,
    wg,
    wu,
    wd,
    sg,
    su,
    sd,
    x_send,
    x_recv,
    part_send,
    part_recv,
    q_heads,
    logit_buf,
    att_heads,
    att_all,
    col_send,
    col_recv,
    coef_all,
    moe_all,
    pair_send,
    pair_recv,
    back_send,
    back_recv,
    local_sem,
    send_sem,
    recv_sem,
    moe_send_sem,
    moe_recv_sem,
    relay_send_sem,
    relay_recv_sem,
    pair_send_sem,
    pair_recv_sem,
    chain_send_sem,
    chain_recv_sem,
):
    me = lax.axis_index("ep")
    chips = n // 2
    chip, core = me // 2, me % 2
    partner = chip * 2 + 1 - core

    def met(step):
        other, bit = chip, 1
        while bit < chips:
            if step & bit:
                other = other + bit * (1 - 2 * (chip // bit % 2))
            bit *= 2
        return other

    def remote(source, target, sent, arrived, device):
        return pltpu.make_async_remote_copy(
            src_ref=source,
            dst_ref=target,
            send_sem=sent,
            recv_sem=arrived,
            device_id={"ep": device},
            device_id_type=pl.DeviceIdType.MESH,
        )

    seqs, width = tokens.shape
    shard = width // n
    groups, places = key_shift.shape[1], key_shift.shape[2]
    heads = head_offset.shape[0]
    per_group = heads // groups
    head_dim = ck.shape[2] // groups
    experts_here = wg.shape[0]

    near = NEAR
    tiers = n // near
    tier, seat = me // near, me % near
    wo = wo_all.at[tier]

    pairs = [
        (tokens_h, tokens),
        (norm_gain_h, norm_gain),
        (wo_h, wo),
        (wk_h, wk),
        (wv_h, wv),
        (wq_h, wq),
        (route_ids_h, route_ids),
        (route_score_h, route_score),
        (head_offset_h, head_offset),
        (lengths_h, lengths),
        (moe_gain_h, moe_gain),
        (ck_h, ck),
        (key_shift_h, key_shift),
        (cv_h, cv),
        (sg_h, sg),
        (su_h, su),
        (sd_h, sd),
        (wg_h, wg),
        (wu_h, wu),
        (wd_h, wd),
    ]
    loads = {}
    for place, (source, target) in enumerate(pairs):
        loads[id(target)] = pltpu.make_async_copy(source, target, local_sem.at[place])

    def ready(target):
        loads[id(target)].wait()

    barrier = pltpu.get_barrier_semaphore()

    def greet(step, carry):
        pl.semaphore_signal(
            barrier,
            inc=1,
            device_id={"ep": lax.rem(me + step, n)},
            device_id_type=pl.DeviceIdType.MESH,
        )
        return carry

    lax.fori_loop(1, n, greet, 0)
    for copy in loads.values():
        copy.start()

    def send_all(source_of, target, phase):
        def body(step, carry):
            peer = lax.rem(me + step, n)
            remote(
                source_of(peer), target.at[me], send_sem.at[phase], recv_sem.at[phase], peer
            ).start()
            return carry

        lax.fori_loop(1, n, body, 0)

    def send_near(source_of, target, phase):
        for step in range(1, near):
            place = (seat + step) % near
            remote(
                source_of(place),
                target.at[seat],
                send_sem.at[phase],
                recv_sem.at[phase],
                tier * near + place,
            ).start()

    def chain(step):
        below, above = tier - step + 1, tier + step - 1
        up = ((tier < tiers - 1) & (below >= 0), below, me + near, 0)
        down = ((tier > 0) & (above < tiers), above, me - near, 1)
        return [
            (
                active,
                lambda held=held, device=device, way=way: remote(
                    wo_all.at[held],
                    wo_all.at[held],
                    chain_send_sem.at[way, step],
                    chain_recv_sem.at[way, step],
                    device,
                ),
            )
            for active, held, device, way in (up, down)
        ]

    def chain_send(step):
        for active, copy in chain(step):
            pl.when(active)(lambda copy=copy: copy().start())

    def chain_sent(step):
        for active, copy in chain(step):
            pl.when(active)(lambda copy=copy: copy().wait_send())

    def chain_wait(step):
        for active, held, way in ((tier >= step, tier - step, 0), (tier + step < tiers, tier + step, 1)):

            def arrived(held=held, way=way):
                block = wo_all.at[held]
                pltpu.make_async_copy(block, block, chain_recv_sem.at[way, step]).wait()

            pl.when(active)(arrived)

    def wait_blocks(target, sem):
        blocks = target.at[pl.ds(0, target.shape[0] - 1)]
        pltpu.make_async_copy(blocks, blocks, sem).wait()

    ready(tokens)
    ready(norm_gain)
    residual_in = tokens[...].astype(F32)
    normed = norm_rows(residual_in, norm_gain[...].astype(F32).reshape(1, width)).astype(BF16)
    for peer in range(n):
        x_send[peer] = normed[:, peer * shard : (peer + 1) * shard]
    x_recv[me] = x_send[me]
    pl.semaphore_wait(barrier, n - 1)
    send_all(lambda peer: x_send.at[peer], x_recv, 0)

    ready(wo)
    chain_send(1)

    ready(route_ids)
    ready(route_score)
    score = route_score[...]
    share = ROUTED_SCALE * score / jnp.sum(score, axis=1, keepdims=True)
    ids = route_ids[...]
    expert_lane = lax.broadcasted_iota(jnp.int32, coef_all.shape[1:], 1)
    table = jnp.zeros(coef_all.shape[1:], F32)
    for pick in range(ids.shape[1]):
        table = table + jnp.where(ids[:, pick : pick + 1] == expert_lane, share[:, pick : pick + 1], 0.0)
    coef_all[me] = table

    ready(wk)
    new_key[...] = dot(normed, wk[...]).astype(BF16)
    ready(wv)
    new_value[...] = dot(normed, wv[...]).astype(BF16)

    ready(wq)
    wait_blocks(x_recv, recv_sem.at[0])
    part_send[...] = dot(stacked(x_recv[...]), wq[...]).reshape(part_send.shape).astype(BF16)
    part_recv[me] = part_send[me]
    send_all(lambda peer: part_send.at[peer], part_recv, 1)

    ready(head_offset)
    ready(lengths)
    ready(moe_gain)
    row = lax.broadcasted_iota(jnp.int32, (heads, 1), 0)
    offset_column = jnp.zeros((heads, 1), F32)
    for head in range(heads):
        offset_column = jnp.where(row == head, head_offset[head], offset_column)
    place_row = lax.broadcasted_iota(jnp.int32, (1, places), 1)
    live_rows = []
    for seq in range(seqs):
        live_rows.append(place_row < lengths[seq])

    if tiers > 1:
        chain_wait(1)
        chain_send(2)
    wait_blocks(part_recv, recv_sem.at[1])
    if tiers > 2:
        chain_wait(2)
        chain_send(3)
    send_all(lambda peer: coef_all.at[me], coef_all, 4)
    queries = jnp.sum(part_recv[...].astype(F32), axis=0).astype(BF16).astype(F32)
    blank = jnp.zeros((seqs, head_dim), F32)
    for head in range(heads):
        pieces = [blank] * groups
        pieces[head // per_group] = queries[:, head * head_dim : (head + 1) * head_dim]
        q_heads[:, head, :] = jnp.concatenate(pieces, axis=1)

    ready(ck)
    ready(key_shift)
    scale = 1.0 / math.sqrt(head_dim)
    for seq in range(seqs):
        product = lax.dot_general(
            q_heads[seq].astype(BF16),
            ck[seq],
            (((1,), (1,)), ((), ())),
            preferred_element_type=F32,
        )
        shift = key_shift[seq]
        shift_rows = jnp.broadcast_to(shift[0:1], (heads, places))
        for group in range(1, groups):
            shift_rows = jnp.where(row // per_group == group, shift[group : group + 1], shift_rows)
        logit_buf[seq] = product * scale + offset_column + shift_rows

    chunk = 128
    later = (
        lax.broadcasted_iota(jnp.int32, (chunk, chunk), 0)
        > lax.broadcasted_iota(jnp.int32, (chunk, chunk), 1)
    ).astype(BF16)
    rows = seqs * heads
    live_count = jnp.concatenate(
        [jnp.full((heads, 1), 0, jnp.int32) + lengths[seq] for seq in range(seqs)], axis=0
    )
    carry = jnp.zeros((rows, 1), F32)
    weights = [None] * (places // chunk)
    for piece in reversed(range(places // chunk)):
        logits = logit_buf[:, :, piece * chunk : (piece + 1) * chunk].reshape(rows, chunk)
        spot = lax.broadcasted_iota(jnp.int32, (rows, chunk), 1) + piece * chunk
        live = spot < live_count
        tail = jnp.log1p(jnp.exp(-jnp.abs(logits)))
        log_take = jnp.minimum(logits, 0.0) - tail
        log_fall = jnp.where(live, jnp.minimum(-logits, 0.0) - tail, 0.0)
        first = log_fall.astype(BF16)
        rest = log_fall - first.astype(F32)
        second = rest.astype(BF16)
        third = (rest - second.astype(F32)).astype(BF16)
        sums = dot(jnp.concatenate([first, second, third], axis=0), later)
        after = (sums[2 * rows :] + sums[rows : 2 * rows]) + sums[:rows] + carry
        weights[piece] = jnp.where(live, jnp.exp(log_take + after), 0.0)
        carry = carry + jnp.sum(log_fall, axis=1, keepdims=True)

    ready(cv)
    for seq in range(seqs):
        own = jnp.concatenate(
            [block[seq * heads : (seq + 1) * heads] for block in weights], axis=1
        ).astype(BF16)
        att_heads[seq] = dot(own, cv[seq])
    pieces = []
    for head in range(heads):
        low = (head // per_group) * head_dim
        pieces.append(att_heads[:, head, :][:, low : low + head_dim])
    att_all[seat] = jnp.concatenate(pieces, axis=1).astype(BF16)
    send_near(lambda place: att_all.at[seat], att_all, 2)

    for step in range(3, tiers):
        chain_wait(step)
        chain_send(step + 1)
    wait_blocks(att_all, recv_sem.at[2])
    att_rows = stacked(att_all[...])
    for other in range(tiers):
        columns = dot(att_rows, wo_all[other]).astype(BF16)
        col_send[:, other] = columns.astype(F32).reshape(near, seqs, shard).astype(BF16)
    col_recv[seat] = col_send[seat]
    send_near(lambda place: col_send.at[place], col_recv, 3)
    wait_blocks(col_recv, recv_sem.at[3])
    branch = jnp.concatenate(
        [col_recv[owner % near, owner // near].astype(F32) for owner in range(n)], axis=1
    )
    residual = residual_in + branch
    moe_in = norm_rows(residual, moe_gain[...].astype(F32).reshape(1, width)).astype(BF16)
    moe_all[me] = moe_in
    relays = [remote(moe_all.at[me], moe_all.at[me], relay_send_sem.at[0], relay_recv_sem.at[0], partner)]
    relays[0].start()
    spread = [None]
    for step in range(1, chips):
        copy = remote(
            moe_all.at[me],
            moe_all.at[me],
            moe_send_sem.at[step],
            moe_recv_sem.at[step],
            met(step) * 2 + core,
        )
        copy.start()
        spread.append(copy)

    ready(sg)
    ready(su)
    ready(sd)
    hidden = jax.nn.silu(dot(moe_in, sg[...])) * dot(moe_in, su[...])
    total = residual + dot(hidden.astype(BF16), sd[...])

    wait_blocks(coef_all, recv_sem.at[4])
    ready(wg)
    ready(wu)
    ready(wd)
    parts = pair_send.shape[0]
    group = chips // parts
    backs, kept = [], []

    def give_back(part):
        backs[part].wait_recv()
        both = kept[part] + pair_recv[part].astype(F32)
        for place in range(group):
            step = part * group + place
            if step == 0:
                continue
            back_send[step - 1] = both[place].astype(BF16)
            remote(
                back_send.at[step - 1],
                back_recv.at[step - 1],
                send_sem.at[5],
                recv_sem.at[5],
                met(step) * 2 + core,
            ).start()
        return both[0]

    for part in range(parts):
        steps = range(part * group, (part + 1) * group)
        for step in steps:
            if step > 0:
                spread[step].wait_recv()
                held = moe_all.at[met(step) * 2 + core]
                copy = remote(held, held, relay_send_sem.at[step], relay_recv_sem.at[step], partner)
                copy.start()
                relays.append(copy)
        if part == 1:
            total = total + give_back(0)
        elif part > 1:
            give_back(part - 1)
        for step in steps:
            relays[step].wait_recv()
        owners = [met(step) * 2 + core for step in steps]
        owners += [met(step) * 2 + 1 - core for step in steps]
        moe_rows = jnp.concatenate([moe_all[owner].astype(F32) for owner in owners], axis=0).astype(BF16)
        coefs = jnp.concatenate([coef_all[owner] for owner in owners], axis=0)
        lane = lax.broadcasted_iota(jnp.int32, coefs.shape, 1)
        mixed = None
        for expert in range(experts_here):
            hidden = jax.nn.silu(dot(moe_rows, wg[expert])) * dot(moe_rows, wu[expert])
            result = dot(hidden.astype(BF16), wd[expert]).astype(BF16).astype(F32)
            mine = lane == me * experts_here + expert
            term = jnp.sum(jnp.where(mine, coefs, 0.0), axis=1, keepdims=True) * result
            mixed = term if mixed is None else mixed + term
        mixed = mixed.reshape(2, group, seqs, width)
        pair_send[part] = mixed[1].astype(BF16)
        copy = remote(
            pair_send.at[part],
            pair_recv.at[part],
            pair_send_sem.at[part],
            pair_recv_sem.at[part],
            partner,
        )
        copy.start()
        backs.append(copy)
        kept.append(mixed[0])
    if parts > 1:
        give_back(parts - 1)
    else:
        total = total + give_back(0)
    pltpu.make_async_copy(back_recv, back_recv, recv_sem.at[5]).wait()
    for step in range(chips - 1):
        total = total + back_recv[step].astype(F32)
    out[...] = total.astype(BF16)

    wait_blocks(x_send, send_sem.at[0])
    wait_blocks(part_send, send_sem.at[1])
    wait_blocks(att_all, send_sem.at[2])
    wait_blocks(col_send, send_sem.at[3])
    wait_blocks(coef_all, send_sem.at[4])
    for step in range(1, tiers):
        chain_sent(step)
    pltpu.make_async_copy(back_send, back_send, send_sem.at[5]).wait()
    for copy in spread[1:] + relays + backs:
        copy.wait_send()


def hand_on_kernel(*refs):
    for source, target in zip(refs[: len(refs) // 2], refs[len(refs) // 2 :]):
        target[...] = source[...]


def shards(
    tokens,
    norm_gain,
    w_query,
    w_key,
    w_value,
    w_out,
    cache_k,
    cache_v,
    head_offset,
    key_shift,
    lengths,
    moe_gain,
    route_ids,
    route_score,
    w_gate,
    w_up,
    w_down,
    shared_gate,
    shared_up,
    shared_down,
):
    n = lax.axis_size("ep")
    seqs, width = tokens.shape
    query_width = w_query.shape[1]
    shard = w_query.shape[0]
    heads = head_offset.shape[0]
    places, kv_width = cache_k.shape[1:]
    experts_here = w_gate.shape[0]
    vmem = pl.BlockSpec(memory_space=pltpu.VMEM)
    hbm = pl.BlockSpec(memory_space=pl.ANY)
    tiers = n // NEAR
    scalars = [head_offset, lengths]
    arrays = [
        tokens,
        norm_gain,
        head_offset,
        lengths,
        moe_gain,
        route_ids,
        route_score,
        key_shift,
        w_query,
        w_key,
        w_value,
        w_out,
        cache_k,
        cache_v,
        w_gate,
        w_up,
        w_down,
        shared_gate,
        shared_up,
        shared_down,
    ]
    held = []
    for array in arrays:
        space = pltpu.SMEM if any(array is scalar for scalar in scalars) else pltpu.VMEM
        shape = (tiers, *array.shape) if array is w_out else array.shape
        held.append(space(shape, array.dtype))
    chips = n // 2
    parts = min(MOE_PARTS, chips)
    out_shape = (
        jax.ShapeDtypeStruct((seqs, width), BF16),
        jax.ShapeDtypeStruct((seqs, w_key.shape[1]), BF16),
        jax.ShapeDtypeStruct((seqs, w_value.shape[1]), BF16),
    )
    results = pl.pallas_call(
        functools.partial(layer_kernel, n),
        out_shape=out_shape,
        in_specs=[hbm] * len(arrays),
        out_specs=(vmem, vmem, vmem),
        scratch_shapes=held
        + [
            pltpu.VMEM((n, seqs, shard), BF16),
            pltpu.VMEM((n, seqs, shard), BF16),
            pltpu.VMEM((n, seqs, query_width), BF16),
            pltpu.VMEM((n, seqs, query_width), BF16),
            pltpu.VMEM((seqs, heads, kv_width), F32),
            pltpu.VMEM((seqs, heads, places), F32),
            pltpu.VMEM((seqs, heads, kv_width), F32),
            pltpu.VMEM((NEAR, seqs, query_width), BF16),
            pltpu.VMEM((NEAR, tiers, seqs, w_out.shape[1]), BF16),
            pltpu.VMEM((NEAR, tiers, seqs, w_out.shape[1]), BF16),
            pltpu.VMEM((n, seqs, n * experts_here), F32),
            pltpu.VMEM((n, seqs, width), BF16),
            pltpu.VMEM((parts, chips // parts, seqs, width), BF16),
            pltpu.VMEM((parts, chips // parts, seqs, width), BF16),
            pltpu.VMEM((chips - 1, seqs, width), BF16),
            pltpu.VMEM((chips - 1, seqs, width), BF16),
            pltpu.SemaphoreType.DMA((len(arrays),)),
            pltpu.SemaphoreType.DMA((6,)),
            pltpu.SemaphoreType.DMA((6,)),
            pltpu.SemaphoreType.DMA((chips,)),
            pltpu.SemaphoreType.DMA((chips,)),
            pltpu.SemaphoreType.DMA((chips,)),
            pltpu.SemaphoreType.DMA((chips,)),
            pltpu.SemaphoreType.DMA((parts,)),
            pltpu.SemaphoreType.DMA((parts,)),
            pltpu.SemaphoreType.DMA((2, tiers + 1)),
            pltpu.SemaphoreType.DMA((2, tiers + 1)),
        ],
        compiler_params=pltpu.CompilerParams(
            collective_id=0, has_side_effects=True, vmem_limit_bytes=60 * 1024 * 1024
        ),
    )(*arrays)
    return pl.pallas_call(
        hand_on_kernel,
        out_shape=out_shape,
        in_specs=[vmem] * 3,
        out_specs=(vmem, vmem, vmem),
    )(*results)


def solution(mesh):
    placed = (
        P(("grp", "ep"), None),
        P(),
        P("ep", None),
        P(),
        P(),
        P(None, "ep"),
        P(("grp", "ep"), None, None),
        P(("grp", "ep"), None, None),
        P(),
        P(("grp", "ep"), None, None),
        P(("grp", "ep")),
        P(),
        P(("grp", "ep"), None),
        P(("grp", "ep"), None),
        P("ep", None, None),
        P("ep", None, None),
        P("ep", None, None),
        P(),
        P(),
        P(),
    )
    return jax.shard_map(
        shards,
        mesh=mesh,
        in_specs=placed,
        out_specs=(P(("grp", "ep"), None), P(("grp", "ep"), None), P(("grp", "ep"), None)),
        check_vma=False,
    )
```

```python
import functools
import math

import jax
import jax.numpy as jnp
from jax import lax
from jax.experimental import pallas as pl
from jax.experimental.pallas import tpu as pltpu
from jax.sharding import PartitionSpec as P

EPSILON = 1e-06
ROUTED_SCALE = 2.5
MOE_PARTS = 4
NEAR = 4
F32 = jnp.float32
BF16 = jnp.bfloat16


def norm_rows(values, gain_row):
    mean_sq = jnp.mean(values * values, axis=-1, keepdims=True)
    return values * lax.rsqrt(mean_sq + EPSILON) * gain_row


def dot(left, right):
    return jnp.dot(left, right, preferred_element_type=F32)


def stacked(blocks):
    count, rows, width = blocks.shape
    return blocks.astype(F32).reshape(count * rows, width).astype(BF16)


def layer_kernel(
    n,
    tokens_h,
    norm_gain_h,
    head_offset_h,
    lengths_h,
    moe_gain_h,
    route_ids_h,
    route_score_h,
    key_shift_h,
    wq_h,
    wk_h,
    wv_h,
    wo_h,
    ck_h,
    cv_h,
    wg_h,
    wu_h,
    wd_h,
    sg_h,
    su_h,
    sd_h,
    out,
    new_key,
    new_value,
    tokens,
    norm_gain,
    head_offset,
    lengths,
    moe_gain,
    route_ids,
    route_score,
    key_shift,
    wq,
    wk,
    wv,
    wo_all,
    ck,
    cv,
    wg,
    wu,
    wd,
    sg,
    su,
    sd,
    x_send,
    x_recv,
    part_send,
    part_recv,
    q_heads,
    logit_buf,
    att_heads,
    att_all,
    col_send,
    col_recv,
    coef_all,
    moe_all,
    pair_send,
    pair_recv,
    back_send,
    back_recv,
    local_sem,
    send_sem,
    recv_sem,
    moe_send_sem,
    moe_recv_sem,
    relay_send_sem,
    relay_recv_sem,
    pair_send_sem,
    pair_recv_sem,
    tier_send_sem,
    tier_recv_sem,
    copy_send_sem,
    copy_recv_sem,
):
    me = lax.axis_index("ep")
    chips = n // 2
    chip, core = me // 2, me % 2
    partner = chip * 2 + 1 - core

    def partner_of(index, step):
        other, bit = index, 1
        while bit <= step:
            if step & bit:
                other = other + bit * (1 - 2 * (index // bit % 2))
            bit *= 2
        return other

    def met(step):
        return partner_of(chip, step)

    def remote(source, target, sent, arrived, device):
        return pltpu.make_async_remote_copy(
            src_ref=source,
            dst_ref=target,
            send_sem=sent,
            recv_sem=arrived,
            device_id={"ep": device},
            device_id_type=pl.DeviceIdType.MESH,
        )

    seqs, width = tokens.shape
    shard = width // n
    groups, places = key_shift.shape[1], key_shift.shape[2]
    heads = head_offset.shape[0]
    per_group = heads // groups
    head_dim = ck.shape[2] // groups
    experts_here = wg.shape[0]

    near = NEAR
    tiers = n // near
    tier, seat = me // near, me % near
    wo = wo_all.at[tier]
    copy_index, copies = lax.axis_index("grp"), wo_all.shape[1]

    pairs = [
        (tokens_h, tokens),
        (norm_gain_h, norm_gain),
        (wo_h, wo),
        (wk_h, wk),
        (wv_h, wv),
        (wq_h, wq),
        (route_ids_h, route_ids),
        (route_score_h, route_score),
        (head_offset_h, head_offset),
        (lengths_h, lengths),
        (moe_gain_h, moe_gain),
        (ck_h, ck),
        (key_shift_h, key_shift),
        (cv_h, cv),
        (sg_h, sg),
        (su_h, su),
        (sd_h, sd),
        (wg_h, wg),
        (wu_h, wu),
        (wd_h, wd),
    ]
    loads = {}
    for place, (source, target) in enumerate(pairs):
        loads[id(target)] = pltpu.make_async_copy(source, target, local_sem.at[place])

    def ready(target):
        loads[id(target)].wait()

    barrier = pltpu.get_barrier_semaphore()

    def greet(step, carry):
        pl.semaphore_signal(
            barrier,
            inc=1,
            device_id={"ep": lax.rem(me + step, n)},
            device_id_type=pl.DeviceIdType.MESH,
        )
        return carry

    lax.fori_loop(1, n, greet, 0)
    for other in range(1, copies):
        pl.semaphore_signal(
            barrier,
            inc=1,
            device_id={"grp": (copy_index + other) % copies},
            device_id_type=pl.DeviceIdType.MESH,
        )
    for copy in loads.values():
        copy.start()

    def send_all(source_of, target, phase):
        def body(step, carry):
            peer = lax.rem(me + step, n)
            remote(
                source_of(peer), target.at[me], send_sem.at[phase], recv_sem.at[phase], peer
            ).start()
            return carry

        lax.fori_loop(1, n, body, 0)

    def send_near(source_of, target, phase):
        for step in range(1, near):
            place = (seat + step) % near
            remote(
                source_of(place),
                target.at[seat],
                send_sem.at[phase],
                recv_sem.at[phase],
                tier * near + place,
            ).start()

    def tier_copy(step):
        mine = wo_all.at[tier, copy_index]
        return remote(
            mine,
            mine,
            tier_send_sem.at[step],
            tier_recv_sem.at[step],
            partner_of(tier, step) * near + seat,
        )

    def to_copies(step):
        made = []
        for other in range(1, copies):
            piece = wo_all.at[partner_of(tier, step), copy_index]
            made.append(
                pltpu.make_async_remote_copy(
                    src_ref=piece,
                    dst_ref=piece,
                    send_sem=copy_send_sem.at[step, other],
                    recv_sem=copy_recv_sem.at[step, other],
                    device_id={"grp": (copy_index + other) % copies},
                    device_id_type=pl.DeviceIdType.MESH,
                )
            )
        return made

    def pass_on(step):
        tier_copy(step).wait_recv()
        for copy in to_copies(step):
            copy.start()

    def wait_blocks(target, sem):
        blocks = target.at[pl.ds(0, target.shape[0] - 1)]
        pltpu.make_async_copy(blocks, blocks, sem).wait()

    ready(tokens)
    ready(norm_gain)
    residual_in = tokens[...].astype(F32)
    normed = norm_rows(residual_in, norm_gain[...].astype(F32).reshape(1, width)).astype(BF16)
    for peer in range(n):
        x_send[peer] = normed[:, peer * shard : (peer + 1) * shard]
    x_recv[me] = x_send[me]
    pl.semaphore_wait(barrier, n - 1 + copies - 1)
    send_all(lambda peer: x_send.at[peer], x_recv, 0)

    ready(wo)
    for step in range(1, tiers):
        tier_copy(step).start()

    ready(route_ids)
    ready(route_score)
    score = route_score[...]
    share = ROUTED_SCALE * score / jnp.sum(score, axis=1, keepdims=True)
    ids = route_ids[...]
    expert_lane = lax.broadcasted_iota(jnp.int32, coef_all.shape[1:], 1)
    table = jnp.zeros(coef_all.shape[1:], F32)
    for pick in range(ids.shape[1]):
        table = table + jnp.where(ids[:, pick : pick + 1] == expert_lane, share[:, pick : pick + 1], 0.0)
    coef_all[me] = table

    ready(wk)
    new_key[...] = dot(normed, wk[...]).astype(BF16)
    ready(wv)
    new_value[...] = dot(normed, wv[...]).astype(BF16)

    ready(wq)
    wait_blocks(x_recv, recv_sem.at[0])
    part_send[...] = dot(stacked(x_recv[...]), wq[...]).reshape(part_send.shape).astype(BF16)
    part_recv[me] = part_send[me]
    send_all(lambda peer: part_send.at[peer], part_recv, 1)

    ready(head_offset)
    ready(lengths)
    ready(moe_gain)
    row = lax.broadcasted_iota(jnp.int32, (heads, 1), 0)
    offset_column = jnp.zeros((heads, 1), F32)
    for head in range(heads):
        offset_column = jnp.where(row == head, head_offset[head], offset_column)
    place_row = lax.broadcasted_iota(jnp.int32, (1, places), 1)
    live_rows = []
    for seq in range(seqs):
        live_rows.append(place_row < lengths[seq])

    for step in range(1, min(tiers, 2)):
        pass_on(step)
    wait_blocks(part_recv, recv_sem.at[1])
    for step in range(2, min(tiers, 3)):
        pass_on(step)
    send_all(lambda peer: coef_all.at[me], coef_all, 4)
    queries = jnp.sum(part_recv[...].astype(F32), axis=0).astype(BF16).astype(F32)
    blank = jnp.zeros((seqs, head_dim), F32)
    for head in range(heads):
        pieces = [blank] * groups
        pieces[head // per_group] = queries[:, head * head_dim : (head + 1) * head_dim]
        q_heads[:, head, :] = jnp.concatenate(pieces, axis=1)

    ready(ck)
    ready(key_shift)
    scale = 1.0 / math.sqrt(head_dim)
    for seq in range(seqs):
        product = lax.dot_general(
            q_heads[seq].astype(BF16),
            ck[seq],
            (((1,), (1,)), ((), ())),
            preferred_element_type=F32,
        )
        shift = key_shift[seq]
        shift_rows = jnp.broadcast_to(shift[0:1], (heads, places))
        for group in range(1, groups):
            shift_rows = jnp.where(row // per_group == group, shift[group : group + 1], shift_rows)
        logit_buf[seq] = product * scale + offset_column + shift_rows

    for step in range(3, tiers):
        pass_on(step)
    chunk = 128
    later = (
        lax.broadcasted_iota(jnp.int32, (chunk, chunk), 0)
        > lax.broadcasted_iota(jnp.int32, (chunk, chunk), 1)
    ).astype(BF16)
    rows = seqs * heads
    live_count = jnp.concatenate(
        [jnp.full((heads, 1), 0, jnp.int32) + lengths[seq] for seq in range(seqs)], axis=0
    )
    carry = jnp.zeros((rows, 1), F32)
    weights = [None] * (places // chunk)
    for piece in reversed(range(places // chunk)):
        logits = logit_buf[:, :, piece * chunk : (piece + 1) * chunk].reshape(rows, chunk)
        spot = lax.broadcasted_iota(jnp.int32, (rows, chunk), 1) + piece * chunk
        live = spot < live_count
        tail = jnp.log1p(jnp.exp(-jnp.abs(logits)))
        log_take = jnp.minimum(logits, 0.0) - tail
        log_fall = jnp.where(live, jnp.minimum(-logits, 0.0) - tail, 0.0)
        first = log_fall.astype(BF16)
        rest = log_fall - first.astype(F32)
        second = rest.astype(BF16)
        third = (rest - second.astype(F32)).astype(BF16)
        sums = dot(jnp.concatenate([first, second, third], axis=0), later)
        after = (sums[2 * rows :] + sums[rows : 2 * rows]) + sums[:rows] + carry
        weights[piece] = jnp.where(live, jnp.exp(log_take + after), 0.0)
        carry = carry + jnp.sum(log_fall, axis=1, keepdims=True)

    ready(cv)
    for seq in range(seqs):
        own = jnp.concatenate(
            [block[seq * heads : (seq + 1) * heads] for block in weights], axis=1
        ).astype(BF16)
        att_heads[seq] = dot(own, cv[seq])
    pieces = []
    for head in range(heads):
        low = (head // per_group) * head_dim
        pieces.append(att_heads[:, head, :][:, low : low + head_dim])
    att_all[seat] = jnp.concatenate(pieces, axis=1).astype(BF16)
    send_near(lambda place: att_all.at[seat], att_all, 2)

    wait_blocks(att_all, recv_sem.at[2])
    att_rows = stacked(att_all[...])
    for step in range(1, tiers):
        for copy in to_copies(step):
            copy.wait_recv()
    for other in range(tiers):
        columns = dot(att_rows, wo_all[other].reshape(att_rows.shape[1], shard)).astype(BF16)
        col_send[:, other] = columns.astype(F32).reshape(near, seqs, shard).astype(BF16)
    col_recv[seat] = col_send[seat]
    send_near(lambda place: col_send.at[place], col_recv, 3)
    wait_blocks(col_recv, recv_sem.at[3])
    branch = jnp.concatenate(
        [col_recv[owner % near, owner // near].astype(F32) for owner in range(n)], axis=1
    )
    residual = residual_in + branch
    moe_in = norm_rows(residual, moe_gain[...].astype(F32).reshape(1, width)).astype(BF16)
    moe_all[me] = moe_in
    relays = [remote(moe_all.at[me], moe_all.at[me], relay_send_sem.at[0], relay_recv_sem.at[0], partner)]
    relays[0].start()
    spread = [None]
    for step in range(1, chips):
        copy = remote(
            moe_all.at[me],
            moe_all.at[me],
            moe_send_sem.at[step],
            moe_recv_sem.at[step],
            met(step) * 2 + core,
        )
        copy.start()
        spread.append(copy)

    ready(sg)
    ready(su)
    ready(sd)
    hidden = jax.nn.silu(dot(moe_in, sg[...])) * dot(moe_in, su[...])
    total = residual + dot(hidden.astype(BF16), sd[...])

    wait_blocks(coef_all, recv_sem.at[4])
    ready(wg)
    ready(wu)
    ready(wd)
    parts = pair_send.shape[0]
    group = chips // parts
    backs, kept = [], []

    def give_back(part):
        backs[part].wait_recv()
        both = kept[part] + pair_recv[part].astype(F32)
        for place in range(group):
            step = part * group + place
            if step == 0:
                continue
            back_send[step - 1] = both[place].astype(BF16)
            remote(
                back_send.at[step - 1],
                back_recv.at[step - 1],
                send_sem.at[5],
                recv_sem.at[5],
                met(step) * 2 + core,
            ).start()
        return both[0]

    for part in range(parts):
        steps = range(part * group, (part + 1) * group)
        for step in steps:
            if step > 0:
                spread[step].wait_recv()
                held = moe_all.at[met(step) * 2 + core]
                copy = remote(held, held, relay_send_sem.at[step], relay_recv_sem.at[step], partner)
                copy.start()
                relays.append(copy)
        if part == 1:
            total = total + give_back(0)
        elif part > 1:
            give_back(part - 1)
        for step in steps:
            relays[step].wait_recv()
        owners = [met(step) * 2 + core for step in steps]
        owners += [met(step) * 2 + 1 - core for step in steps]
        moe_rows = jnp.concatenate([moe_all[owner].astype(F32) for owner in owners], axis=0).astype(BF16)
        coefs = jnp.concatenate([coef_all[owner] for owner in owners], axis=0)
        lane = lax.broadcasted_iota(jnp.int32, coefs.shape, 1)
        mixed = None
        for expert in range(experts_here):
            hidden = jax.nn.silu(dot(moe_rows, wg[expert])) * dot(moe_rows, wu[expert])
            result = dot(hidden.astype(BF16), wd[expert]).astype(BF16).astype(F32)
            mine = lane == me * experts_here + expert
            term = jnp.sum(jnp.where(mine, coefs, 0.0), axis=1, keepdims=True) * result
            mixed = term if mixed is None else mixed + term
        mixed = mixed.reshape(2, group, seqs, width)
        pair_send[part] = mixed[1].astype(BF16)
        copy = remote(
            pair_send.at[part],
            pair_recv.at[part],
            pair_send_sem.at[part],
            pair_recv_sem.at[part],
            partner,
        )
        copy.start()
        backs.append(copy)
        kept.append(mixed[0])
    if parts > 1:
        give_back(parts - 1)
    else:
        total = total + give_back(0)
    pltpu.make_async_copy(back_recv, back_recv, recv_sem.at[5]).wait()
    for step in range(chips - 1):
        total = total + back_recv[step].astype(F32)
    out[...] = total.astype(BF16)

    wait_blocks(x_send, send_sem.at[0])
    wait_blocks(part_send, send_sem.at[1])
    wait_blocks(att_all, send_sem.at[2])
    wait_blocks(col_send, send_sem.at[3])
    wait_blocks(coef_all, send_sem.at[4])
    for step in range(1, tiers):
        tier_copy(step).wait_send()
        for copy in to_copies(step):
            copy.wait_send()
    pltpu.make_async_copy(back_send, back_send, send_sem.at[5]).wait()
    for copy in spread[1:] + relays + backs:
        copy.wait_send()


def hand_on_kernel(*refs):
    for source, target in zip(refs[: len(refs) // 2], refs[len(refs) // 2 :]):
        target[...] = source[...]


def shards(
    tokens,
    norm_gain,
    w_query,
    w_key,
    w_value,
    w_out,
    cache_k,
    cache_v,
    head_offset,
    key_shift,
    lengths,
    moe_gain,
    route_ids,
    route_score,
    w_gate,
    w_up,
    w_down,
    shared_gate,
    shared_up,
    shared_down,
):
    n = lax.axis_size("ep")
    seqs, width = tokens.shape
    query_width = w_query.shape[1]
    shard = w_query.shape[0]
    heads = head_offset.shape[0]
    places, kv_width = cache_k.shape[1:]
    experts_here = w_gate.shape[0]
    vmem = pl.BlockSpec(memory_space=pltpu.VMEM)
    hbm = pl.BlockSpec(memory_space=pl.ANY)
    tiers = n // NEAR
    copies = lax.axis_size("grp")
    out_pieces = w_out.reshape(copies, w_out.shape[0] // copies, w_out.shape[1])
    scalars = [head_offset, lengths]
    arrays = [
        tokens,
        norm_gain,
        head_offset,
        lengths,
        moe_gain,
        route_ids,
        route_score,
        key_shift,
        w_query,
        w_key,
        w_value,
        out_pieces,
        cache_k,
        cache_v,
        w_gate,
        w_up,
        w_down,
        shared_gate,
        shared_up,
        shared_down,
    ]
    held = []
    for array in arrays:
        space = pltpu.SMEM if any(array is scalar for scalar in scalars) else pltpu.VMEM
        shape = (tiers, *array.shape) if array is out_pieces else array.shape
        held.append(space(shape, array.dtype))
    chips = n // 2
    parts = min(MOE_PARTS, chips)
    out_shape = (
        jax.ShapeDtypeStruct((seqs, width), BF16),
        jax.ShapeDtypeStruct((seqs, w_key.shape[1]), BF16),
        jax.ShapeDtypeStruct((seqs, w_value.shape[1]), BF16),
    )
    results = pl.pallas_call(
        functools.partial(layer_kernel, n),
        out_shape=out_shape,
        in_specs=[hbm] * len(arrays),
        out_specs=(vmem, vmem, vmem),
        scratch_shapes=held
        + [
            pltpu.VMEM((n, seqs, shard), BF16),
            pltpu.VMEM((n, seqs, shard), BF16),
            pltpu.VMEM((n, seqs, query_width), BF16),
            pltpu.VMEM((n, seqs, query_width), BF16),
            pltpu.VMEM((seqs, heads, kv_width), F32),
            pltpu.VMEM((seqs, heads, places), F32),
            pltpu.VMEM((seqs, heads, kv_width), F32),
            pltpu.VMEM((NEAR, seqs, query_width), BF16),
            pltpu.VMEM((NEAR, tiers, seqs, w_out.shape[1]), BF16),
            pltpu.VMEM((NEAR, tiers, seqs, w_out.shape[1]), BF16),
            pltpu.VMEM((n, seqs, n * experts_here), F32),
            pltpu.VMEM((n, seqs, width), BF16),
            pltpu.VMEM((parts, chips // parts, seqs, width), BF16),
            pltpu.VMEM((parts, chips // parts, seqs, width), BF16),
            pltpu.VMEM((chips - 1, seqs, width), BF16),
            pltpu.VMEM((chips - 1, seqs, width), BF16),
            pltpu.SemaphoreType.DMA((len(arrays),)),
            pltpu.SemaphoreType.DMA((6,)),
            pltpu.SemaphoreType.DMA((6,)),
            pltpu.SemaphoreType.DMA((chips,)),
            pltpu.SemaphoreType.DMA((chips,)),
            pltpu.SemaphoreType.DMA((chips,)),
            pltpu.SemaphoreType.DMA((chips,)),
            pltpu.SemaphoreType.DMA((parts,)),
            pltpu.SemaphoreType.DMA((parts,)),
            pltpu.SemaphoreType.DMA((tiers,)),
            pltpu.SemaphoreType.DMA((tiers,)),
            pltpu.SemaphoreType.DMA((tiers, copies)),
            pltpu.SemaphoreType.DMA((tiers, copies)),
        ],
        compiler_params=pltpu.CompilerParams(
            collective_id=0, has_side_effects=True, vmem_limit_bytes=60 * 1024 * 1024
        ),
    )(*arrays)
    return pl.pallas_call(
        hand_on_kernel,
        out_shape=out_shape,
        in_specs=[vmem] * 3,
        out_specs=(vmem, vmem, vmem),
    )(*results)


def solution(mesh):
    placed = (
        P(("grp", "ep"), None),
        P(),
        P("ep", None),
        P(),
        P(),
        P(None, "ep"),
        P(("grp", "ep"), None, None),
        P(("grp", "ep"), None, None),
        P(),
        P(("grp", "ep"), None, None),
        P(("grp", "ep")),
        P(),
        P(("grp", "ep"), None),
        P(("grp", "ep"), None),
        P("ep", None, None),
        P("ep", None, None),
        P("ep", None, None),
        P(),
        P(),
        P(),
    )
    return jax.shard_map(
        shards,
        mesh=mesh,
        in_specs=placed,
        out_specs=(P(("grp", "ep"), None), P(("grp", "ep"), None), P(("grp", "ep"), None)),
        check_vma=False,
    )
```

```python
import functools
import math

import jax
import jax.numpy as jnp
from jax import lax
from jax.experimental import pallas as pl
from jax.experimental.pallas import tpu as pltpu
from jax.sharding import PartitionSpec as P

EPSILON = 1e-06
ROUTED_SCALE = 2.5
MOE_PARTS = 4
NEAR = 4
F32 = jnp.float32
BF16 = jnp.bfloat16


def norm_rows(values, gain_row):
    mean_sq = jnp.mean(values * values, axis=-1, keepdims=True)
    return values * lax.rsqrt(mean_sq + EPSILON) * gain_row


def dot(left, right):
    return jnp.dot(left, right, preferred_element_type=F32)


def stacked(blocks):
    count, rows, width = blocks.shape
    return blocks.astype(F32).reshape(count * rows, width).astype(BF16)


def layer_kernel(
    n,
    tokens_h,
    norm_gain_h,
    head_offset_h,
    lengths_h,
    moe_gain_h,
    route_ids_h,
    route_score_h,
    key_shift_h,
    wq_h,
    wk_h,
    wv_h,
    wo_h,
    ck_h,
    cv_h,
    wg_h,
    wu_h,
    wd_h,
    sg_h,
    su_h,
    sd_h,
    out,
    new_key,
    new_value,
    tokens,
    norm_gain,
    head_offset,
    lengths,
    moe_gain,
    route_ids,
    route_score,
    key_shift,
    wq,
    wk,
    wv,
    wo_all,
    ck,
    cv,
    wg,
    wu,
    wd,
    sg,
    su,
    sd,
    x_send,
    x_recv,
    part_send,
    part_recv,
    q_heads,
    logit_buf,
    att_heads,
    att_all,
    col_send,
    col_recv,
    coef_all,
    moe_all,
    pair_send,
    pair_recv,
    back_send,
    back_recv,
    local_sem,
    send_sem,
    recv_sem,
    moe_send_sem,
    moe_recv_sem,
    relay_send_sem,
    relay_recv_sem,
    pair_send_sem,
    pair_recv_sem,
    tier_send_sem,
    tier_recv_sem,
    copy_send_sem,
    copy_recv_sem,
):
    me = lax.axis_index("ep")
    chips = n // 2
    chip, core = me // 2, me % 2
    partner = chip * 2 + 1 - core

    def partner_of(index, step):
        other, bit = index, 1
        while bit <= step:
            if step & bit:
                other = other + bit * (1 - 2 * (index // bit % 2))
            bit *= 2
        return other

    def met(step):
        return partner_of(chip, step)

    def remote(source, target, sent, arrived, device):
        return pltpu.make_async_remote_copy(
            src_ref=source,
            dst_ref=target,
            send_sem=sent,
            recv_sem=arrived,
            device_id={"ep": device},
            device_id_type=pl.DeviceIdType.MESH,
        )

    seqs, width = tokens.shape
    shard = width // n
    groups, places = key_shift.shape[1], key_shift.shape[2]
    heads = head_offset.shape[0]
    per_group = heads // groups
    head_dim = ck.shape[2] // groups
    experts_here = wg.shape[0]

    near = NEAR
    tiers = n // near
    tier, seat = me // near, me % near
    wo = wo_all.at[tier]
    copy_index, copies = lax.axis_index("grp"), wo_all.shape[1]

    pairs = [
        (tokens_h, tokens),
        (norm_gain_h, norm_gain),
        (wo_h, wo),
        (wk_h, wk),
        (wv_h, wv),
        (wq_h, wq),
        (route_ids_h, route_ids),
        (route_score_h, route_score),
        (head_offset_h, head_offset),
        (lengths_h, lengths),
        (moe_gain_h, moe_gain),
        (ck_h, ck),
        (key_shift_h, key_shift),
        (cv_h, cv),
        (sg_h, sg),
        (su_h, su),
        (sd_h, sd),
        (wg_h, wg),
        (wu_h, wu),
        (wd_h, wd),
    ]
    loads = {}
    for place, (source, target) in enumerate(pairs):
        loads[id(target)] = pltpu.make_async_copy(source, target, local_sem.at[place])

    def ready(target):
        loads[id(target)].wait()

    barrier = pltpu.get_barrier_semaphore()

    def greet(step, carry):
        pl.semaphore_signal(
            barrier,
            inc=1,
            device_id={"ep": lax.rem(me + step, n)},
            device_id_type=pl.DeviceIdType.MESH,
        )
        return carry

    lax.fori_loop(1, n, greet, 0)
    for other in range(1, copies):
        pl.semaphore_signal(
            barrier,
            inc=1,
            device_id={"grp": (copy_index + other) % copies},
            device_id_type=pl.DeviceIdType.MESH,
        )
    for copy in loads.values():
        copy.start()

    def send_all(source_of, target, phase):
        def body(step, carry):
            peer = lax.rem(me + step, n)
            remote(
                source_of(peer), target.at[me], send_sem.at[phase], recv_sem.at[phase], peer
            ).start()
            return carry

        lax.fori_loop(1, n, body, 0)

    def send_near(source_of, target, phase):
        for step in range(1, near):
            place = (seat + step) % near
            remote(
                source_of(place),
                target.at[seat],
                send_sem.at[phase],
                recv_sem.at[phase],
                tier * near + place,
            ).start()

    def tier_copy(step):
        mine = wo_all.at[tier, copy_index]
        return remote(
            mine,
            mine,
            tier_send_sem.at[step],
            tier_recv_sem.at[step],
            partner_of(tier, step) * near + seat,
        )

    def to_copies(step):
        made = []
        for other in range(1, copies):
            piece = wo_all.at[partner_of(tier, step), copy_index]
            made.append(
                pltpu.make_async_remote_copy(
                    src_ref=piece,
                    dst_ref=piece,
                    send_sem=copy_send_sem.at[step, other],
                    recv_sem=copy_recv_sem.at[step, other],
                    device_id={"grp": (copy_index + other) % copies},
                    device_id_type=pl.DeviceIdType.MESH,
                )
            )
        return made

    def pass_on(step):
        tier_copy(step).wait_recv()
        for copy in to_copies(step):
            copy.start()

    def wait_blocks(target, sem):
        blocks = target.at[pl.ds(0, target.shape[0] - 1)]
        pltpu.make_async_copy(blocks, blocks, sem).wait()

    ready(tokens)
    ready(norm_gain)
    residual_in = tokens[...].astype(F32)
    normed = norm_rows(residual_in, norm_gain[...].astype(F32).reshape(1, width)).astype(BF16)
    for peer in range(n):
        x_send[peer] = normed[:, peer * shard : (peer + 1) * shard]
    x_recv[me] = x_send[me]
    pl.semaphore_wait(barrier, n - 1 + copies - 1)
    send_all(lambda peer: x_send.at[peer], x_recv, 0)

    ready(wo)
    for step in range(1, tiers):
        tier_copy(step).start()

    ready(route_ids)
    ready(route_score)
    score = route_score[...]
    share = ROUTED_SCALE * score / jnp.sum(score, axis=1, keepdims=True)
    ids = route_ids[...]
    expert_lane = lax.broadcasted_iota(jnp.int32, coef_all.shape[1:], 1)
    table = jnp.zeros(coef_all.shape[1:], F32)
    for pick in range(ids.shape[1]):
        table = table + jnp.where(ids[:, pick : pick + 1] == expert_lane, share[:, pick : pick + 1], 0.0)
    coef_all[me] = table

    ready(wk)
    new_key[...] = dot(normed, wk[...]).astype(BF16)
    ready(wv)
    new_value[...] = dot(normed, wv[...]).astype(BF16)

    ready(wq)
    wait_blocks(x_recv, recv_sem.at[0])
    part_send[...] = dot(stacked(x_recv[...]), wq[...]).reshape(part_send.shape).astype(BF16)
    part_recv[me] = part_send[me]
    send_all(lambda peer: part_send.at[peer], part_recv, 1)

    ready(head_offset)
    ready(lengths)
    ready(moe_gain)
    row = lax.broadcasted_iota(jnp.int32, (heads, 1), 0)
    offset_column = jnp.zeros((heads, 1), F32)
    for head in range(heads):
        offset_column = jnp.where(row == head, head_offset[head], offset_column)
    place_row = lax.broadcasted_iota(jnp.int32, (1, places), 1)
    live_rows = []
    for seq in range(seqs):
        live_rows.append(place_row < lengths[seq])

    for step in range(1, min(tiers, 2)):
        pass_on(step)
    wait_blocks(part_recv, recv_sem.at[1])
    for step in range(2, min(tiers, 3)):
        pass_on(step)
    queries = jnp.sum(part_recv[...].astype(F32), axis=0).astype(BF16).astype(F32)
    blank = jnp.zeros((seqs, head_dim), F32)
    for head in range(heads):
        pieces = [blank] * groups
        pieces[head // per_group] = queries[:, head * head_dim : (head + 1) * head_dim]
        q_heads[:, head, :] = jnp.concatenate(pieces, axis=1)

    ready(ck)
    ready(key_shift)
    scale = 1.0 / math.sqrt(head_dim)
    for seq in range(seqs):
        product = lax.dot_general(
            q_heads[seq].astype(BF16),
            ck[seq],
            (((1,), (1,)), ((), ())),
            preferred_element_type=F32,
        )
        shift = key_shift[seq]
        shift_rows = jnp.broadcast_to(shift[0:1], (heads, places))
        for group in range(1, groups):
            shift_rows = jnp.where(row // per_group == group, shift[group : group + 1], shift_rows)
        logit_buf[seq] = product * scale + offset_column + shift_rows

    for step in range(3, tiers):
        pass_on(step)
    chunk = 128
    later = (
        lax.broadcasted_iota(jnp.int32, (chunk, chunk), 0)
        > lax.broadcasted_iota(jnp.int32, (chunk, chunk), 1)
    ).astype(BF16)
    rows = seqs * heads
    live_count = jnp.concatenate(
        [jnp.full((heads, 1), 0, jnp.int32) + lengths[seq] for seq in range(seqs)], axis=0
    )
    carry = jnp.zeros((rows, 1), F32)
    weights = [None] * (places // chunk)
    for piece in reversed(range(places // chunk)):
        logits = logit_buf[:, :, piece * chunk : (piece + 1) * chunk].reshape(rows, chunk)
        spot = lax.broadcasted_iota(jnp.int32, (rows, chunk), 1) + piece * chunk
        live = spot < live_count
        tail = jnp.log1p(jnp.exp(-jnp.abs(logits)))
        log_take = jnp.minimum(logits, 0.0) - tail
        log_fall = jnp.where(live, jnp.minimum(-logits, 0.0) - tail, 0.0)
        first = log_fall.astype(BF16)
        rest = log_fall - first.astype(F32)
        second = rest.astype(BF16)
        third = (rest - second.astype(F32)).astype(BF16)
        sums = dot(jnp.concatenate([first, second, third], axis=0), later)
        after = (sums[2 * rows :] + sums[rows : 2 * rows]) + sums[:rows] + carry
        weights[piece] = jnp.where(live, jnp.exp(log_take + after), 0.0)
        carry = carry + jnp.sum(log_fall, axis=1, keepdims=True)

    ready(cv)
    for seq in range(seqs):
        own = jnp.concatenate(
            [block[seq * heads : (seq + 1) * heads] for block in weights], axis=1
        ).astype(BF16)
        att_heads[seq] = dot(own, cv[seq])
    pieces = []
    for head in range(heads):
        low = (head // per_group) * head_dim
        pieces.append(att_heads[:, head, :][:, low : low + head_dim])
    att_all[seat] = jnp.concatenate(pieces, axis=1).astype(BF16)
    send_near(lambda place: att_all.at[seat], att_all, 2)
    send_all(lambda peer: coef_all.at[me], coef_all, 4)

    wait_blocks(att_all, recv_sem.at[2])
    att_rows = stacked(att_all[...])
    for step in range(1, tiers):
        for copy in to_copies(step):
            copy.wait_recv()
    for other in range(tiers):
        columns = dot(att_rows, wo_all[other].reshape(att_rows.shape[1], shard)).astype(BF16)
        col_send[:, other] = columns.astype(F32).reshape(near, seqs, shard).astype(BF16)
    col_recv[seat] = col_send[seat]
    send_near(lambda place: col_send.at[place], col_recv, 3)
    wait_blocks(col_recv, recv_sem.at[3])
    branch = jnp.concatenate(
        [col_recv[owner % near, owner // near].astype(F32) for owner in range(n)], axis=1
    )
    residual = residual_in + branch
    moe_in = norm_rows(residual, moe_gain[...].astype(F32).reshape(1, width)).astype(BF16)
    moe_all[me] = moe_in
    relays = [remote(moe_all.at[me], moe_all.at[me], relay_send_sem.at[0], relay_recv_sem.at[0], partner)]
    relays[0].start()
    spread = [None]
    for step in range(1, chips):
        copy = remote(
            moe_all.at[me],
            moe_all.at[me],
            moe_send_sem.at[step],
            moe_recv_sem.at[step],
            met(step) * 2 + core,
        )
        copy.start()
        spread.append(copy)

    ready(sg)
    ready(su)
    ready(sd)
    hidden = jax.nn.silu(dot(moe_in, sg[...])) * dot(moe_in, su[...])
    total = residual + dot(hidden.astype(BF16), sd[...])

    wait_blocks(coef_all, recv_sem.at[4])
    ready(wg)
    ready(wu)
    ready(wd)
    parts = pair_send.shape[0]
    group = chips // parts
    backs, kept = [], []

    def give_back(part):
        backs[part].wait_recv()
        both = kept[part] + pair_recv[part].astype(F32)
        for place in range(group):
            step = part * group + place
            if step == 0:
                continue
            back_send[step - 1] = both[place].astype(BF16)
            remote(
                back_send.at[step - 1],
                back_recv.at[step - 1],
                send_sem.at[5],
                recv_sem.at[5],
                met(step) * 2 + core,
            ).start()
        return both[0]

    def take_in(part):
        for step in range(part * group, (part + 1) * group):
            if step > 0:
                spread[step].wait_recv()
                held = moe_all.at[met(step) * 2 + core]
                copy = remote(held, held, relay_send_sem.at[step], relay_recv_sem.at[step], partner)
                copy.start()
                relays.append(copy)

    take_in(0)
    for part in range(parts):
        if part + 1 < parts:
            take_in(part + 1)
        steps = range(part * group, (part + 1) * group)
        for step in steps:
            relays[step].wait_recv()
        owners = [met(step) * 2 + core for step in steps]
        owners += [met(step) * 2 + 1 - core for step in steps]
        moe_rows = jnp.concatenate([moe_all[owner].astype(F32) for owner in owners], axis=0).astype(BF16)
        coefs = jnp.concatenate([coef_all[owner] for owner in owners], axis=0)
        lane = lax.broadcasted_iota(jnp.int32, coefs.shape, 1)
        mixed = None
        for expert in range(experts_here):
            hidden = jax.nn.silu(dot(moe_rows, wg[expert])) * dot(moe_rows, wu[expert])
            result = dot(hidden.astype(BF16), wd[expert]).astype(BF16).astype(F32)
            mine = lane == me * experts_here + expert
            term = jnp.sum(jnp.where(mine, coefs, 0.0), axis=1, keepdims=True) * result
            mixed = term if mixed is None else mixed + term
        mixed = mixed.reshape(2, group, seqs, width)
        pair_send[part] = mixed[1].astype(BF16)
        copy = remote(
            pair_send.at[part],
            pair_recv.at[part],
            pair_send_sem.at[part],
            pair_recv_sem.at[part],
            partner,
        )
        copy.start()
        backs.append(copy)
        kept.append(mixed[0])
        if part == 1:
            total = total + give_back(0)
        elif part > 1:
            give_back(part - 1)
    if parts > 1:
        give_back(parts - 1)
    else:
        total = total + give_back(0)
    pltpu.make_async_copy(back_recv, back_recv, recv_sem.at[5]).wait()
    for step in range(chips - 1):
        total = total + back_recv[step].astype(F32)
    out[...] = total.astype(BF16)

    wait_blocks(x_send, send_sem.at[0])
    wait_blocks(part_send, send_sem.at[1])
    wait_blocks(att_all, send_sem.at[2])
    wait_blocks(col_send, send_sem.at[3])
    wait_blocks(coef_all, send_sem.at[4])
    for step in range(1, tiers):
        tier_copy(step).wait_send()
        for copy in to_copies(step):
            copy.wait_send()
    pltpu.make_async_copy(back_send, back_send, send_sem.at[5]).wait()
    for copy in spread[1:] + relays + backs:
        copy.wait_send()


def hand_on_kernel(*refs):
    for source, target in zip(refs[: len(refs) // 2], refs[len(refs) // 2 :]):
        target[...] = source[...]


def shards(
    tokens,
    norm_gain,
    w_query,
    w_key,
    w_value,
    w_out,
    cache_k,
    cache_v,
    head_offset,
    key_shift,
    lengths,
    moe_gain,
    route_ids,
    route_score,
    w_gate,
    w_up,
    w_down,
    shared_gate,
    shared_up,
    shared_down,
):
    n = lax.axis_size("ep")
    seqs, width = tokens.shape
    query_width = w_query.shape[1]
    shard = w_query.shape[0]
    heads = head_offset.shape[0]
    places, kv_width = cache_k.shape[1:]
    experts_here = w_gate.shape[0]
    vmem = pl.BlockSpec(memory_space=pltpu.VMEM)
    hbm = pl.BlockSpec(memory_space=pl.ANY)
    tiers = n // NEAR
    copies = lax.axis_size("grp")
    out_pieces = w_out.reshape(copies, w_out.shape[0] // copies, w_out.shape[1])
    scalars = [head_offset, lengths]
    arrays = [
        tokens,
        norm_gain,
        head_offset,
        lengths,
        moe_gain,
        route_ids,
        route_score,
        key_shift,
        w_query,
        w_key,
        w_value,
        out_pieces,
        cache_k,
        cache_v,
        w_gate,
        w_up,
        w_down,
        shared_gate,
        shared_up,
        shared_down,
    ]
    held = []
    for array in arrays:
        space = pltpu.SMEM if any(array is scalar for scalar in scalars) else pltpu.VMEM
        shape = (tiers, *array.shape) if array is out_pieces else array.shape
        held.append(space(shape, array.dtype))
    chips = n // 2
    parts = min(MOE_PARTS, chips)
    out_shape = (
        jax.ShapeDtypeStruct((seqs, width), BF16),
        jax.ShapeDtypeStruct((seqs, w_key.shape[1]), BF16),
        jax.ShapeDtypeStruct((seqs, w_value.shape[1]), BF16),
    )
    results = pl.pallas_call(
        functools.partial(layer_kernel, n),
        out_shape=out_shape,
        in_specs=[hbm] * len(arrays),
        out_specs=(vmem, vmem, vmem),
        scratch_shapes=held
        + [
            pltpu.VMEM((n, seqs, shard), BF16),
            pltpu.VMEM((n, seqs, shard), BF16),
            pltpu.VMEM((n, seqs, query_width), BF16),
            pltpu.VMEM((n, seqs, query_width), BF16),
            pltpu.VMEM((seqs, heads, kv_width), F32),
            pltpu.VMEM((seqs, heads, places), F32),
            pltpu.VMEM((seqs, heads, kv_width), F32),
            pltpu.VMEM((NEAR, seqs, query_width), BF16),
            pltpu.VMEM((NEAR, tiers, seqs, w_out.shape[1]), BF16),
            pltpu.VMEM((NEAR, tiers, seqs, w_out.shape[1]), BF16),
            pltpu.VMEM((n, seqs, n * experts_here), F32),
            pltpu.VMEM((n, seqs, width), BF16),
            pltpu.VMEM((parts, chips // parts, seqs, width), BF16),
            pltpu.VMEM((parts, chips // parts, seqs, width), BF16),
            pltpu.VMEM((chips - 1, seqs, width), BF16),
            pltpu.VMEM((chips - 1, seqs, width), BF16),
            pltpu.SemaphoreType.DMA((len(arrays),)),
            pltpu.SemaphoreType.DMA((6,)),
            pltpu.SemaphoreType.DMA((6,)),
            pltpu.SemaphoreType.DMA((chips,)),
            pltpu.SemaphoreType.DMA((chips,)),
            pltpu.SemaphoreType.DMA((chips,)),
            pltpu.SemaphoreType.DMA((chips,)),
            pltpu.SemaphoreType.DMA((parts,)),
            pltpu.SemaphoreType.DMA((parts,)),
            pltpu.SemaphoreType.DMA((tiers,)),
            pltpu.SemaphoreType.DMA((tiers,)),
            pltpu.SemaphoreType.DMA((tiers, copies)),
            pltpu.SemaphoreType.DMA((tiers, copies)),
        ],
        compiler_params=pltpu.CompilerParams(
            collective_id=0, has_side_effects=True, vmem_limit_bytes=60 * 1024 * 1024
        ),
    )(*arrays)
    return pl.pallas_call(
        hand_on_kernel,
        out_shape=out_shape,
        in_specs=[vmem] * 3,
        out_specs=(vmem, vmem, vmem),
    )(*results)


def solution(mesh):
    placed = (
        P(("grp", "ep"), None),
        P(),
        P("ep", None),
        P(),
        P(),
        P(None, "ep"),
        P(("grp", "ep"), None, None),
        P(("grp", "ep"), None, None),
        P(),
        P(("grp", "ep"), None, None),
        P(("grp", "ep")),
        P(),
        P(("grp", "ep"), None),
        P(("grp", "ep"), None),
        P("ep", None, None),
        P("ep", None, None),
        P("ep", None, None),
        P(),
        P(),
        P(),
    )
    return jax.shard_map(
        shards,
        mesh=mesh,
        in_specs=placed,
        out_specs=(P(("grp", "ep"), None), P(("grp", "ep"), None), P(("grp", "ep"), None)),
        check_vma=False,
    )
```

```python
import functools
import math

import jax
import jax.numpy as jnp
from jax import lax
from jax.experimental import pallas as pl
from jax.experimental.pallas import tpu as pltpu
from jax.sharding import PartitionSpec as P

EPSILON = 1e-06
ROUTED_SCALE = 2.5
MOE_PARTS = 4
NEAR = 4
F32 = jnp.float32
BF16 = jnp.bfloat16


def norm_rows(values, gain_row):
    mean_sq = jnp.mean(values * values, axis=-1, keepdims=True)
    return values * lax.rsqrt(mean_sq + EPSILON) * gain_row


def dot(left, right):
    return jnp.dot(left, right, preferred_element_type=F32)


def stacked(blocks):
    count, rows, width = blocks.shape
    return blocks.astype(F32).reshape(count * rows, width).astype(BF16)


def layer_kernel(
    n,
    tokens_h,
    norm_gain_h,
    head_offset_h,
    lengths_h,
    moe_gain_h,
    route_ids_h,
    route_score_h,
    key_shift_h,
    wq_h,
    wk_h,
    wv_h,
    wo_h,
    ck_h,
    cv_h,
    wg_h,
    wu_h,
    wd_h,
    sg_h,
    su_h,
    sd_h,
    out,
    new_key,
    new_value,
    tokens,
    norm_gain,
    head_offset,
    lengths,
    moe_gain,
    route_ids,
    route_score,
    key_shift,
    wq,
    wk,
    wv,
    wo_all,
    ck,
    cv,
    wg,
    wu,
    wd,
    sg,
    su,
    sd,
    x_send,
    x_recv,
    part_send,
    part_recv,
    q_heads,
    logit_buf,
    att_heads,
    att_all,
    col_send,
    col_recv,
    coef_all,
    moe_all,
    pair_send,
    pair_recv,
    back_send,
    back_recv,
    local_sem,
    send_sem,
    recv_sem,
    moe_send_sem,
    moe_recv_sem,
    relay_send_sem,
    relay_recv_sem,
    pair_send_sem,
    pair_recv_sem,
    chain_send_sem,
    chain_recv_sem,
):
    me = lax.axis_index("ep")
    chips = n // 2
    chip, core = me // 2, me % 2
    partner = chip * 2 + 1 - core

    def met(step):
        other, bit = chip, 1
        while bit < chips:
            if step & bit:
                other = other + bit * (1 - 2 * (chip // bit % 2))
            bit *= 2
        return other

    def remote(source, target, sent, arrived, device):
        return pltpu.make_async_remote_copy(
            src_ref=source,
            dst_ref=target,
            send_sem=sent,
            recv_sem=arrived,
            device_id={"ep": device},
            device_id_type=pl.DeviceIdType.MESH,
        )

    seqs, width = tokens.shape
    shard = width // n
    groups, places = key_shift.shape[1], key_shift.shape[2]
    heads = head_offset.shape[0]
    per_group = heads // groups
    head_dim = ck.shape[2] // groups
    experts_here = wg.shape[0]

    near = NEAR
    tiers = n // near
    tier, seat = me // near, me % near
    wo = wo_all.at[tier]

    pairs = [
        (tokens_h, tokens),
        (norm_gain_h, norm_gain),
        (wo_h, wo),
        (wk_h, wk),
        (wv_h, wv),
        (wq_h, wq),
        (route_ids_h, route_ids),
        (route_score_h, route_score),
        (head_offset_h, head_offset),
        (lengths_h, lengths),
        (moe_gain_h, moe_gain),
        (ck_h, ck),
        (key_shift_h, key_shift),
        (cv_h, cv),
        (sg_h, sg),
        (su_h, su),
        (sd_h, sd),
        (wg_h, wg),
        (wu_h, wu),
        (wd_h, wd),
    ]
    loads = {}
    for place, (source, target) in enumerate(pairs):
        loads[id(target)] = pltpu.make_async_copy(source, target, local_sem.at[place])

    def ready(target):
        loads[id(target)].wait()

    barrier = pltpu.get_barrier_semaphore()

    def greet(step, carry):
        pl.semaphore_signal(
            barrier,
            inc=1,
            device_id={"ep": lax.rem(me + step, n)},
            device_id_type=pl.DeviceIdType.MESH,
        )
        return carry

    lax.fori_loop(1, n, greet, 0)
    for copy in loads.values():
        copy.start()

    def send_all(source_of, target, phase):
        def body(step, carry):
            peer = lax.rem(me + step, n)
            remote(
                source_of(peer), target.at[me], send_sem.at[phase], recv_sem.at[phase], peer
            ).start()
            return carry

        lax.fori_loop(1, n, body, 0)

    def send_near(source_of, target, phase):
        for step in range(1, near):
            place = (seat + step) % near
            remote(
                source_of(place),
                target.at[seat],
                send_sem.at[phase],
                recv_sem.at[phase],
                tier * near + place,
            ).start()

    def chain(step):
        below, above = tier - step + 1, tier + step - 1
        up = ((tier < tiers - 1) & (below >= 0), below, me + near, 0)
        down = ((tier > 0) & (above < tiers), above, me - near, 1)
        return [
            (
                active,
                lambda held=held, device=device, way=way: remote(
                    wo_all.at[held],
                    wo_all.at[held],
                    chain_send_sem.at[way, step],
                    chain_recv_sem.at[way, step],
                    device,
                ),
            )
            for active, held, device, way in (up, down)
        ]

    def chain_send(step):
        for active, copy in chain(step):
            pl.when(active)(lambda copy=copy: copy().start())

    def chain_sent(step):
        for active, copy in chain(step):
            pl.when(active)(lambda copy=copy: copy().wait_send())

    def chain_wait(step):
        for active, held, way in ((tier >= step, tier - step, 0), (tier + step < tiers, tier + step, 1)):

            def arrived(held=held, way=way):
                block = wo_all.at[held]
                pltpu.make_async_copy(block, block, chain_recv_sem.at[way, step]).wait()

            pl.when(active)(arrived)

    def wait_blocks(target, sem):
        blocks = target.at[pl.ds(0, target.shape[0] - 1)]
        pltpu.make_async_copy(blocks, blocks, sem).wait()

    ready(tokens)
    ready(norm_gain)
    residual_in = tokens[...].astype(F32)
    normed = norm_rows(residual_in, norm_gain[...].astype(F32).reshape(1, width)).astype(BF16)
    for peer in range(n):
        x_send[peer] = normed[:, peer * shard : (peer + 1) * shard]
    x_recv[me] = x_send[me]
    pl.semaphore_wait(barrier, n - 1)
    send_all(lambda peer: x_send.at[peer], x_recv, 0)

    ready(wo)
    chain_send(1)

    ready(route_ids)
    ready(route_score)
    score = route_score[...]
    share = ROUTED_SCALE * score / jnp.sum(score, axis=1, keepdims=True)
    ids = route_ids[...]
    expert_lane = lax.broadcasted_iota(jnp.int32, coef_all.shape[1:], 1)
    table = jnp.zeros(coef_all.shape[1:], F32)
    for pick in range(ids.shape[1]):
        table = table + jnp.where(ids[:, pick : pick + 1] == expert_lane, share[:, pick : pick + 1], 0.0)
    coef_all[me] = table

    ready(wk)
    new_key[...] = dot(normed, wk[...]).astype(BF16)
    ready(wv)
    new_value[...] = dot(normed, wv[...]).astype(BF16)

    ready(wq)
    wait_blocks(x_recv, recv_sem.at[0])
    part_send[...] = dot(stacked(x_recv[...]), wq[...]).reshape(part_send.shape).astype(BF16)
    part_recv[me] = part_send[me]
    send_all(lambda peer: part_send.at[peer], part_recv, 1)

    ready(head_offset)
    ready(lengths)
    ready(moe_gain)
    row = lax.broadcasted_iota(jnp.int32, (heads, 1), 0)
    offset_column = jnp.zeros((heads, 1), F32)
    for head in range(heads):
        offset_column = jnp.where(row == head, head_offset[head], offset_column)
    place_row = lax.broadcasted_iota(jnp.int32, (1, places), 1)
    live_rows = []
    for seq in range(seqs):
        live_rows.append(place_row < lengths[seq])

    if tiers > 1:
        chain_wait(1)
        chain_send(2)
    wait_blocks(part_recv, recv_sem.at[1])
    queries = jnp.sum(part_recv[...].astype(F32), axis=0).astype(BF16).astype(F32)
    blank = jnp.zeros((seqs, head_dim), F32)
    for head in range(heads):
        pieces = [blank] * groups
        pieces[head // per_group] = queries[:, head * head_dim : (head + 1) * head_dim]
        q_heads[:, head, :] = jnp.concatenate(pieces, axis=1)

    ready(ck)
    ready(key_shift)
    scale = 1.0 / math.sqrt(head_dim)
    for seq in range(seqs):
        product = lax.dot_general(
            q_heads[seq].astype(BF16),
            ck[seq],
            (((1,), (1,)), ((), ())),
            preferred_element_type=F32,
        )
        shift = key_shift[seq]
        shift_rows = jnp.broadcast_to(shift[0:1], (heads, places))
        for group in range(1, groups):
            shift_rows = jnp.where(row // per_group == group, shift[group : group + 1], shift_rows)
        logit_buf[seq] = product * scale + offset_column + shift_rows

    if tiers > 2:
        chain_wait(2)
        chain_send(3)
    chunk = 128
    later = (
        lax.broadcasted_iota(jnp.int32, (chunk, chunk), 0)
        > lax.broadcasted_iota(jnp.int32, (chunk, chunk), 1)
    ).astype(BF16)
    rows = seqs * heads
    live_count = jnp.concatenate(
        [jnp.full((heads, 1), 0, jnp.int32) + lengths[seq] for seq in range(seqs)], axis=0
    )
    carry = jnp.zeros((rows, 1), F32)
    weights = [None] * (places // chunk)
    for piece in reversed(range(places // chunk)):
        logits = logit_buf[:, :, piece * chunk : (piece + 1) * chunk].reshape(rows, chunk)
        spot = lax.broadcasted_iota(jnp.int32, (rows, chunk), 1) + piece * chunk
        live = spot < live_count
        tail = jnp.log1p(jnp.exp(-jnp.abs(logits)))
        log_take = jnp.minimum(logits, 0.0) - tail
        log_fall = jnp.where(live, jnp.minimum(-logits, 0.0) - tail, 0.0)
        first = log_fall.astype(BF16)
        rest = log_fall - first.astype(F32)
        second = rest.astype(BF16)
        third = (rest - second.astype(F32)).astype(BF16)
        sums = dot(jnp.concatenate([first, second, third], axis=0), later)
        after = (sums[2 * rows :] + sums[rows : 2 * rows]) + sums[:rows] + carry
        weights[piece] = jnp.where(live, jnp.exp(log_take + after), 0.0)
        carry = carry + jnp.sum(log_fall, axis=1, keepdims=True)

    ready(cv)
    for seq in range(seqs):
        own = jnp.concatenate(
            [block[seq * heads : (seq + 1) * heads] for block in weights], axis=1
        ).astype(BF16)
        att_heads[seq] = dot(own, cv[seq])
    pieces = []
    for head in range(heads):
        low = (head // per_group) * head_dim
        pieces.append(att_heads[:, head, :][:, low : low + head_dim])
    att_all[seat] = jnp.concatenate(pieces, axis=1).astype(BF16)
    send_near(lambda place: att_all.at[seat], att_all, 2)

    for step in range(3, tiers):
        chain_wait(step)
        chain_send(step + 1)
    wait_blocks(att_all, recv_sem.at[2])
    att_rows = stacked(att_all[...])
    for other in range(tiers):
        columns = dot(att_rows, wo_all[other]).astype(BF16)
        col_send[:, other] = columns.astype(F32).reshape(near, seqs, shard).astype(BF16)
    col_recv[seat] = col_send[seat]
    send_near(lambda place: col_send.at[place], col_recv, 3)
    send_all(lambda peer: coef_all.at[me], coef_all, 4)
    wait_blocks(col_recv, recv_sem.at[3])
    branch = jnp.concatenate(
        [col_recv[owner % near, owner // near].astype(F32) for owner in range(n)], axis=1
    )
    residual = residual_in + branch
    moe_in = norm_rows(residual, moe_gain[...].astype(F32).reshape(1, width)).astype(BF16)
    moe_all[me] = moe_in
    relays = [remote(moe_all.at[me], moe_all.at[me], relay_send_sem.at[0], relay_recv_sem.at[0], partner)]
    relays[0].start()
    spread = [None]
    for step in range(1, chips):
        copy = remote(
            moe_all.at[me],
            moe_all.at[me],
            moe_send_sem.at[step],
            moe_recv_sem.at[step],
            met(step) * 2 + core,
        )
        copy.start()
        spread.append(copy)

    ready(sg)
    ready(su)
    ready(sd)
    hidden = jax.nn.silu(dot(moe_in, sg[...])) * dot(moe_in, su[...])
    total = residual + dot(hidden.astype(BF16), sd[...])

    wait_blocks(coef_all, recv_sem.at[4])
    ready(wg)
    ready(wu)
    ready(wd)
    parts = pair_send.shape[0]
    group = chips // parts
    backs, kept = [], []

    def give_back(part):
        backs[part].wait_recv()
        both = kept[part] + pair_recv[part].astype(F32)
        for place in range(group):
            step = part * group + place
            if step == 0:
                continue
            back_send[step - 1] = both[place].astype(BF16)
            remote(
                back_send.at[step - 1],
                back_recv.at[step - 1],
                send_sem.at[5],
                recv_sem.at[5],
                met(step) * 2 + core,
            ).start()
        return both[0]

    for part in range(parts):
        steps = range(part * group, (part + 1) * group)
        for step in steps:
            if step > 0:
                spread[step].wait_recv()
                held = moe_all.at[met(step) * 2 + core]
                copy = remote(held, held, relay_send_sem.at[step], relay_recv_sem.at[step], partner)
                copy.start()
                relays.append(copy)
        if part == 1:
            total = total + give_back(0)
        elif part > 1:
            give_back(part - 1)
        for step in steps:
            relays[step].wait_recv()
        owners = [met(step) * 2 + core for step in steps]
        owners += [met(step) * 2 + 1 - core for step in steps]
        moe_rows = jnp.concatenate([moe_all[owner].astype(F32) for owner in owners], axis=0).astype(BF16)
        coefs = jnp.concatenate([coef_all[owner] for owner in owners], axis=0)
        lane = lax.broadcasted_iota(jnp.int32, coefs.shape, 1)
        mixed = None
        for expert in range(experts_here):
            hidden = jax.nn.silu(dot(moe_rows, wg[expert])) * dot(moe_rows, wu[expert])
            result = dot(hidden.astype(BF16), wd[expert]).astype(BF16).astype(F32)
            mine = lane == me * experts_here + expert
            term = jnp.sum(jnp.where(mine, coefs, 0.0), axis=1, keepdims=True) * result
            mixed = term if mixed is None else mixed + term
        mixed = mixed.reshape(2, group, seqs, width)
        pair_send[part] = mixed[1].astype(BF16)
        copy = remote(
            pair_send.at[part],
            pair_recv.at[part],
            pair_send_sem.at[part],
            pair_recv_sem.at[part],
            partner,
        )
        copy.start()
        backs.append(copy)
        kept.append(mixed[0])
    if parts > 1:
        give_back(parts - 1)
    else:
        total = total + give_back(0)
    pltpu.make_async_copy(back_recv, back_recv, recv_sem.at[5]).wait()
    for step in range(chips - 1):
        total = total + back_recv[step].astype(F32)
    out[...] = total.astype(BF16)

    wait_blocks(x_send, send_sem.at[0])
    wait_blocks(part_send, send_sem.at[1])
    wait_blocks(att_all, send_sem.at[2])
    wait_blocks(col_send, send_sem.at[3])
    wait_blocks(coef_all, send_sem.at[4])
    for step in range(1, tiers):
        chain_sent(step)
    pltpu.make_async_copy(back_send, back_send, send_sem.at[5]).wait()
    for copy in spread[1:] + relays + backs:
        copy.wait_send()


def hand_on_kernel(*refs):
    for source, target in zip(refs[: len(refs) // 2], refs[len(refs) // 2 :]):
        target[...] = source[...]


def shards(
    tokens,
    norm_gain,
    w_query,
    w_key,
    w_value,
    w_out,
    cache_k,
    cache_v,
    head_offset,
    key_shift,
    lengths,
    moe_gain,
    route_ids,
    route_score,
    w_gate,
    w_up,
    w_down,
    shared_gate,
    shared_up,
    shared_down,
):
    n = lax.axis_size("ep")
    seqs, width = tokens.shape
    query_width = w_query.shape[1]
    shard = w_query.shape[0]
    heads = head_offset.shape[0]
    places, kv_width = cache_k.shape[1:]
    experts_here = w_gate.shape[0]
    vmem = pl.BlockSpec(memory_space=pltpu.VMEM)
    hbm = pl.BlockSpec(memory_space=pl.ANY)
    tiers = n // NEAR
    scalars = [head_offset, lengths]
    arrays = [
        tokens,
        norm_gain,
        head_offset,
        lengths,
        moe_gain,
        route_ids,
        route_score,
        key_shift,
        w_query,
        w_key,
        w_value,
        w_out,
        cache_k,
        cache_v,
        w_gate,
        w_up,
        w_down,
        shared_gate,
        shared_up,
        shared_down,
    ]
    held = []
    for array in arrays:
        space = pltpu.SMEM if any(array is scalar for scalar in scalars) else pltpu.VMEM
        shape = (tiers, *array.shape) if array is w_out else array.shape
        held.append(space(shape, array.dtype))
    chips = n // 2
    parts = min(MOE_PARTS, chips)
    out_shape = (
        jax.ShapeDtypeStruct((seqs, width), BF16),
        jax.ShapeDtypeStruct((seqs, w_key.shape[1]), BF16),
        jax.ShapeDtypeStruct((seqs, w_value.shape[1]), BF16),
    )
    results = pl.pallas_call(
        functools.partial(layer_kernel, n),
        out_shape=out_shape,
        in_specs=[hbm] * len(arrays),
        out_specs=(vmem, vmem, vmem),
        scratch_shapes=held
        + [
            pltpu.VMEM((n, seqs, shard), BF16),
            pltpu.VMEM((n, seqs, shard), BF16),
            pltpu.VMEM((n, seqs, query_width), BF16),
            pltpu.VMEM((n, seqs, query_width), BF16),
            pltpu.VMEM((seqs, heads, kv_width), F32),
            pltpu.VMEM((seqs, heads, places), F32),
            pltpu.VMEM((seqs, heads, kv_width), F32),
            pltpu.VMEM((NEAR, seqs, query_width), BF16),
            pltpu.VMEM((NEAR, tiers, seqs, w_out.shape[1]), BF16),
            pltpu.VMEM((NEAR, tiers, seqs, w_out.shape[1]), BF16),
            pltpu.VMEM((n, seqs, n * experts_here), F32),
            pltpu.VMEM((n, seqs, width), BF16),
            pltpu.VMEM((parts, chips // parts, seqs, width), BF16),
            pltpu.VMEM((parts, chips // parts, seqs, width), BF16),
            pltpu.VMEM((chips - 1, seqs, width), BF16),
            pltpu.VMEM((chips - 1, seqs, width), BF16),
            pltpu.SemaphoreType.DMA((len(arrays),)),
            pltpu.SemaphoreType.DMA((6,)),
            pltpu.SemaphoreType.DMA((6,)),
            pltpu.SemaphoreType.DMA((chips,)),
            pltpu.SemaphoreType.DMA((chips,)),
            pltpu.SemaphoreType.DMA((chips,)),
            pltpu.SemaphoreType.DMA((chips,)),
            pltpu.SemaphoreType.DMA((parts,)),
            pltpu.SemaphoreType.DMA((parts,)),
            pltpu.SemaphoreType.DMA((2, tiers + 1)),
            pltpu.SemaphoreType.DMA((2, tiers + 1)),
        ],
        compiler_params=pltpu.CompilerParams(
            collective_id=0, has_side_effects=True, vmem_limit_bytes=60 * 1024 * 1024
        ),
    )(*arrays)
    return pl.pallas_call(
        hand_on_kernel,
        out_shape=out_shape,
        in_specs=[vmem] * 3,
        out_specs=(vmem, vmem, vmem),
    )(*results)


def solution(mesh):
    placed = (
        P(("grp", "ep"), None),
        P(),
        P("ep", None),
        P(),
        P(),
        P(None, "ep"),
        P(("grp", "ep"), None, None),
        P(("grp", "ep"), None, None),
        P(),
        P(("grp", "ep"), None, None),
        P(("grp", "ep")),
        P(),
        P(("grp", "ep"), None),
        P(("grp", "ep"), None),
        P("ep", None, None),
        P("ep", None, None),
        P("ep", None, None),
        P(),
        P(),
        P(),
    )
    return jax.shard_map(
        shards,
        mesh=mesh,
        in_specs=placed,
        out_specs=(P(("grp", "ep"), None), P(("grp", "ep"), None), P(("grp", "ep"), None)),
        check_vma=False,
    )
```
